32 devices in a mesh: grp: 2 (over y), ep: 4 (over z), tp: 4 (over x, core).
Axes of the slice: x: 2, y: 2, z: 4, core: 2. Of those that a mesh axis runs over, the one named last changes fastest.
Arguments:
- outer_gate: bfloat16 [2048, 2048], P(('grp', 'ep'), 'tp'), parts along dimension 0, may hold values from -6 to 6
- inner_gate: bfloat16 [2048, 2048], P(('grp', 'ep'), 'tp'), parts along dimension 0, may hold values from -6 to 6
- inner_value: bfloat16 [2048, 2048], P(('grp', 'ep'), 'tp'), parts along dimension 0, may hold values from -6 to 6
- conv_taps: bfloat16 [3, 2048], replicated, may hold values from -3 to 3
- mixer_out: bfloat16 [2048, 2048], P('tp'), may hold values from -0.125 to 0.125
- mixer_gain: float32 [2048], replicated, may hold values from 0.1 to 1.9
- moe_tokens: bfloat16 [2048, 2048], P(('grp', 'ep', 'tp')), parts along dimension 0, may hold values from -6 to 6
- expert_gain: float32 [2048], replicated, may hold values from 0.1 to 1.9
- route_ids: int32 [2048, 4], P(('grp', 'ep', 'tp')), parts along dimension 0, may hold values from 0 to 15, all different within a row; in each aligned block of 64 rows (0 to 63, 64 to 127, ...) at most 24 rows name the same one
- route_weights: float32 [2048, 4], P(('grp', 'ep', 'tp')), parts along dimension 0, may hold values from 0.2 to 1
- expert_gate: bfloat16 [16, 2048, 512], P(('ep', 'tp')), may hold values from -0.125 to 0.125
- expert_up: bfloat16 [16, 2048, 512], P(('ep', 'tp')), may hold values from -0.125 to 0.125
- expert_down: bfloat16 [16, 512, 2048], P(('ep', 'tp')), may hold values from -0.25 to 0.25
- shared_gate: bfloat16 [2048, 512], P(None, 'tp'), may hold values from -0.125 to 0.125
- shared_up: bfloat16 [2048, 512], P(None, 'tp'), may hold values from -0.125 to 0.125
- shared_down: bfloat16 [512, 2048], P('tp'), may hold values from -0.25 to 0.25
Outputs:
- mixed_rows: bfloat16 [2048, 2048], P(('grp', 'ep', 'tp')), parts along dimension 0
- expert_rows: bfloat16 [2048, 2048], P(('grp', 'ep', 'tp')), parts along dimension 0
The draws below stay inside these ranges and needn't reach their ends.
There are 2 independent parts, one for each index of `grp`. The reference program is written for one: setup_inputs(seed, part) draws one part's arguments, and reference() takes and returns one part's arrays. A program takes and returns all parts, laid end to end along the dimension named above; an argument that names none is the same for every part. Nothing has to cross between parts.
Inputs may be any that keep to these rules, and one draw needn't show every extreme that they name: `route_ids`: each row names 4 different experts; among the 64 rows of one device (aligned blocks) no expert is named more than 24 times, a bound that some block reaches.
All inputs are finite; a program needn't handle non-finite values.
Results may differ from the reference program's by a relative error of at most 0.012.
Values may be sent and summed in bfloat16 or wider, within the bound.
A program may use at most 64 MiB of HBM per device.

```python
import math
import jax
import jax.numpy as jnp
import numpy as np
from jax import lax

D = 2048
F = 512
DS = 512
TOP_K = 4
TOK_DEV = 64
EXPERTS = 16
CAP = 24
TOK_A = 1024
TOK_B = 1024
N_EP = 4
N_TP = 4


def block_scale(key, extent, pieces, low, high):
    def one(dim, blocks):
        steps = jax.random.uniform(jax.random.fold_in(jax.random.fold_in(key, 6), dim), (blocks,), jnp.float32, low / len(pieces), high / len(pieces))
        return jnp.repeat(jnp.exp(steps), extent[dim] // blocks).reshape((-1,) + (1,) * (len(extent) - dim - 1))

    gain = one(*pieces[0])
    for cut in pieces[1:]:
        gain = gain * one(*cut)
    return gain


def routed_block(key, own, number, rows, number_of, top, limit, skew):
    sequence = jax.random.permutation(key, number_of)
    packed, common = shares(number_of, rows * top, limit, skew, True), shares(number_of, rows * top, limit, skew, False)
    places = jnp.arange(number_of)

    def named(tallies, offset_by):
        used = int((tallies > 0).sum())
        fixed = max(1, used // 4)
        passed = fixed + (places - fixed + offset_by * (used - fixed)) % max(1, number_of - fixed)
        return jnp.zeros((number_of,), jnp.int32).at[sequence[jnp.where(places < fixed, places, passed)]].set(jnp.asarray(tallies, jnp.int32))

    tallies = jnp.where(number % 4 == 0, named(packed, number // 4), named(common, number - number // 4 - 1))
    mixed = jax.random.permutation(jax.random.fold_in(own, 3), number_of)
    source_of, taker = mixed[0:number_of // 2 * 2:2], mixed[1:number_of // 2 * 2:2]
    room = jnp.minimum(tallies[source_of] - 1, limit - tallies[taker]) // 2
    room = jnp.where((source_of == sequence[0]) | (taker == sequence[0]) | (tallies[taker] == 0), 0, jnp.maximum(room, 0))
    passed = jax.random.randint(jax.random.fold_in(own, 4), (number_of // 2,), 0, 1 << 20) % (room + 1)
    tallies = tallies.at[source_of].add(-passed).at[taker].add(passed)
    labels = jnp.searchsorted(jnp.cumsum(tallies), jnp.arange(rows * top), side="right").astype(jnp.int32)
    listing = labels.reshape(top, rows).T
    listing = listing[jax.random.permutation(jax.random.fold_in(own, 1), rows)]
    offset_by = jax.random.randint(jax.random.fold_in(own, 2), (rows, 1), 0, top)
    return jnp.take_along_axis(listing, (jnp.arange(top)[None, :] + offset_by) % top, axis=1)


def shares(amount, total, bound, slope, full):
    loads = [(1 << 20) // math.isqrt(rank ** slope) + 1 for rank in range(1, amount + 1)]
    largest = bound if full else min(bound, max(-(-total // amount), total * loads[0] // sum(loads)))
    least = 1 if total - largest >= amount - 1 else 0
    given, surplus = [largest] + [least] * (amount - 1), total - largest - least * (amount - 1)
    while surplus > 0:
        movable = [i for i in range(1, amount) if given[i] < largest] or [i for i in range(1, amount) if given[i] < bound]
        mass, remaining = sum([loads[i] for i in movable]), surplus
        for i in movable:
            extra = min(bound - given[i], max(1, remaining * loads[i] // mass), surplus)
            given[i] = given[i] + extra
            surplus = surplus - extra
    return np.array(given)


def centred(key, dims, deviation, bound, shards=(), kind=jnp.bfloat16):
    factor_of = block_scale(key, dims, shards, -0.22, 0.18) if shards else 1.0
    array = jax.random.normal(key, dims, jnp.float32) * deviation * factor_of
    return jnp.minimum(jnp.maximum(array, -bound), bound).astype(kind)


def setup_inputs(seed: int = 0, part: int = 0) -> dict:
    seeds = jax.random.split(jax.random.key(seed), 17)
    part_splits = jax.random.split(jax.random.fold_in(seeds[16], part), 17)
    outer_gate = centred(part_splits[0], (TOK_A, D), 1.0, 6.0, ((0, 4), (1, 4)))
    inner_gate = centred(part_splits[1], (TOK_A, D), 1.0, 6.0, ((0, 4), (1, 4)))
    inner_value = centred(part_splits[2], (TOK_A, D), 1.0, 6.0, ((0, 4), (1, 4)))
    conv_taps = centred(seeds[3], (3, D), 0.577, 3.0)
    mixer_out = centred(seeds[4], (D, D), D ** -0.5, 0.125, ((0, 4),))
    mixer_gain = jnp.clip(1.0 + 0.18 * jax.random.normal(seeds[5], (D,), jnp.float32), 0.1, 1.9)
    moe_tokens = centred(part_splits[6], (TOK_B, D), 1.0, 6.0, ((0, 16),))
    expert_gain = jnp.clip(1.0 + 0.18 * jax.random.normal(seeds[7], (D,), jnp.float32), 0.1, 1.9)
    route_ids_keys = jax.random.split(jax.random.fold_in(part_splits[8], 1), TOK_B // TOK_DEV)
    route_ids_turns = jax.random.permutation(jax.random.fold_in(part_splits[8], 3), TOK_B // TOK_DEV)
    route_ids = jax.vmap(lambda own, number: routed_block(jax.random.fold_in(part_splits[8], 2), own, number, TOK_DEV, EXPERTS, TOP_K, CAP, 2))(route_ids_keys, route_ids_turns).reshape((TOK_B, TOP_K))
    route_weights = jnp.clip(jnp.exp(math.log(1.0) - 1.609438 * jax.random.uniform(part_splits[9], (TOK_B, TOP_K), jnp.float32) ** block_scale(part_splits[9], (TOK_B, TOP_K), ((0, 16),), -0.2, 0.2)), 0.2, 1.0)
    expert_gate = centred(seeds[10], (EXPERTS, D, F), D ** -0.5, 0.125, ((0, 16),))
    expert_up = centred(seeds[11], (EXPERTS, D, F), D ** -0.5, 0.125, ((0, 16),))
    expert_down = centred(seeds[12], (EXPERTS, F, D), F ** -0.5, 0.25, ((0, 16),))
    shared_gate = centred(seeds[13], (D, DS), D ** -0.5, 0.125, ((1, 4),))
    shared_up = centred(seeds[14], (D, DS), D ** -0.5, 0.125, ((1, 4),))
    shared_down = centred(seeds[15], (DS, D), DS ** -0.5, 0.25, ((0, 4),))
    return {"outer_gate": outer_gate, "inner_gate": inner_gate, "inner_value": inner_value, "conv_taps": conv_taps, "mixer_out": mixer_out, "mixer_gain": mixer_gain, "moe_tokens": moe_tokens, "expert_gain": expert_gain, "route_ids": route_ids, "route_weights": route_weights, "expert_gate": expert_gate, "expert_up": expert_up, "expert_down": expert_down, "shared_gate": shared_gate, "shared_up": shared_up, "shared_down": shared_down}


EPSILON = 1e-06

def rms_scale(values, gains):
    return values * lax.rsqrt(lax.optimization_barrier(jnp.mean(values * values, axis=-1, keepdims=True)) + EPSILON) * gains

def reference(outer_gate, inner_gate, inner_value, conv_taps, mixer_out, mixer_gain, moe_tokens, expert_gain, route_ids, route_weights, expert_gate, expert_up, expert_down, shared_gate, shared_up, shared_down):
    kernel = conv_taps.astype(jnp.float32)
    product = inner_gate.astype(jnp.float32) * inner_value.astype(jnp.float32)
    padded = jnp.concatenate([jnp.zeros((2, product.shape[1]), jnp.float32), product], axis=0)
    filtered = kernel[0] * padded[:-2] + kernel[1] * padded[1:-1] + kernel[2] * padded[2:]
    scaled = (outer_gate.astype(jnp.float32) * filtered).astype(jnp.bfloat16)
    shard_width = D // N_TP
    summed = jnp.zeros((scaled.shape[0], D), jnp.float32)
    for shard_index in range(N_TP):
        low = shard_index * shard_width
        partial_sum = jnp.dot(scaled[:, low:low + shard_width], mixer_out[low:low + shard_width], preferred_element_type=jnp.float32)
        rounded = lax.optimization_barrier(partial_sum.astype(jnp.bfloat16))
        summed = summed + rounded.astype(jnp.float32)
    mixed_rows = rms_scale(summed, mixer_gain.astype(jnp.float32)).astype(jnp.bfloat16)
    normed = rms_scale(moe_tokens.astype(jnp.float32), expert_gain.astype(jnp.float32)).astype(jnp.bfloat16)
    token_total = normed.shape[0]
    flat_ids = route_ids.reshape(-1).astype(jnp.int32)
    onehot = (flat_ids[:, None] == jnp.arange(EXPERTS, dtype=jnp.int32)[None, :]).astype(jnp.int32)
    slot_rank = lax.optimization_barrier(jnp.sum((jnp.cumsum(onehot, axis=0, dtype=jnp.int32) - onehot) * onehot, axis=1, dtype=jnp.int32))
    token_of = jnp.arange(flat_ids.shape[0], dtype=jnp.int32) // TOP_K
    slot_count = N_EP * N_TP * CAP
    target = flat_ids * slot_count + slot_rank
    slot_token = jnp.full((EXPERTS * slot_count,), token_total, jnp.int32).at[target].set(token_of).reshape(EXPERTS, slot_count)
    slot_weight = jnp.zeros((EXPERTS * slot_count,), jnp.float32).at[target].set(route_weights.reshape(-1).astype(jnp.float32)).reshape(EXPERTS, slot_count)
    padded_rows = jnp.concatenate([normed, jnp.zeros((1, D), jnp.bfloat16)], axis=0)

    def expert_step(routed, inputs):
        gate_weight, up_weight, down_weight, tokens_here, weights_here = inputs
        chosen = padded_rows[tokens_here]
        gate_value = jnp.dot(chosen, gate_weight, preferred_element_type=jnp.float32)
        up_value = jnp.dot(chosen, up_weight, preferred_element_type=jnp.float32)
        active = (jax.nn.silu(gate_value) * up_value).astype(jnp.bfloat16)
        result = jnp.dot(active, down_weight, preferred_element_type=jnp.float32)
        result = lax.optimization_barrier(result.astype(jnp.bfloat16)).astype(jnp.float32)
        return (routed.at[tokens_here].add(weights_here[:, None] * result), None)
    routed, unused = lax.scan(expert_step, jnp.zeros((token_total + 1, D), jnp.float32), (expert_gate, expert_up, expert_down, slot_token, slot_weight))
    shared_gate_value = jnp.dot(normed, shared_gate, preferred_element_type=jnp.float32)
    shared_up_value = jnp.dot(normed, shared_up, preferred_element_type=jnp.float32)
    shared_act = (jax.nn.silu(shared_gate_value) * shared_up_value).astype(jnp.bfloat16)
    hidden_width = DS // N_TP
    shared_out = jnp.zeros((token_total, D), jnp.float32)
    for shard_index in range(N_TP):
        low = shard_index * hidden_width
        partial_sum = jnp.dot(shared_act[:, low:low + hidden_width], shared_down[low:low + hidden_width], preferred_element_type=jnp.float32)
        rounded = lax.optimization_barrier(partial_sum.astype(jnp.bfloat16))
        shared_out = shared_out + rounded.astype(jnp.float32)
    expert_rows = (routed[:token_total] + shared_out).astype(jnp.bfloat16)
    return (mixed_rows, expert_rows)
```

```python
import functools
import jax
import jax.numpy as jnp
from jax import lax
from jax.experimental import pallas as pl
from jax.experimental.pallas import tpu as pltpu
from jax.sharding import PartitionSpec as P

EPSILON = 1e-06


def passed_along(array, axis, by):
    size = lax.axis_size(axis)
    pairs = [(i, i + by) for i in range(size) if 0 <= i + by < size]
    return lax.ppermute(array, axis, pairs)


def rms_scale(values, gains):
    return values * lax.rsqrt(jnp.mean(values * values, axis=-1, keepdims=True) + EPSILON) * gains


def on_device(
    outer_gate,
    inner_gate,
    inner_value,
    conv_taps,
    mixer_out,
    mixer_gain,
    moe_tokens,
    expert_gain,
    route_ids,
    route_weights,
    expert_gate,
    expert_up,
    expert_down,
    shared_gate,
    shared_up,
    shared_down,
):
    columns = inner_gate.shape[1]
    kernel = lax.dynamic_slice_in_dim(conv_taps, lax.axis_index("tp") * columns, columns, 1).astype(
        jnp.float32
    )
    before_gate, before_value = passed_along((inner_gate[-2:], inner_value[-2:]), "ep", 1)
    gate_rows = jnp.concatenate([before_gate, inner_gate], axis=0).astype(jnp.float32)
    value_rows = jnp.concatenate([before_value, inner_value], axis=0).astype(jnp.float32)
    product = gate_rows * value_rows
    filtered = kernel[0] * product[:-2] + kernel[1] * product[1:-1] + kernel[2] * product[2:]
    scaled = (outer_gate.astype(jnp.float32) * filtered).astype(jnp.bfloat16)
    normed = rms_scale(moe_tokens.astype(jnp.float32), expert_gain).astype(jnp.bfloat16)
    feature_width = normed.shape[1]
    piece = lax.all_gather(normed, "tp", axis=0, tiled=True)
    gate_value = jnp.dot(piece, shared_gate, preferred_element_type=jnp.float32)
    up_value = jnp.dot(piece, shared_up, preferred_element_type=jnp.float32)
    shared_act = (jax.nn.silu(gate_value) * up_value).astype(jnp.bfloat16)
    mixer_part = jnp.dot(scaled, mixer_out, preferred_element_type=jnp.float32)
    shared_part = jnp.dot(shared_act, shared_down, preferred_element_type=jnp.float32)
    both_sums = lax.psum_scatter(
        jnp.concatenate([mixer_part, shared_part], axis=1).astype(jnp.bfloat16),
        "tp",
        scatter_dimension=0,
        tiled=True,
    ).astype(jnp.float32)
    mixed_rows = rms_scale(both_sums[:, :feature_width], mixer_gain).astype(jnp.bfloat16)
    shared_out = both_sums[:, feature_width:]
    row_count, top_count = route_ids.shape
    ep_count = lax.axis_size("ep")
    tp_count = lax.axis_size("tp")
    expert_count = ep_count * tp_count
    capacity = (3 * row_count * top_count + 2 * expert_count - 1) // (2 * expert_count)
    flat_ids = route_ids.reshape(-1)
    onehot = (flat_ids[:, None] == jnp.arange(expert_count, dtype=jnp.int32)[None, :]).astype(
        jnp.int32
    )
    slot_rank = jnp.sum(
        (jnp.cumsum(onehot, axis=0, dtype=jnp.int32) - onehot) * onehot, axis=1, dtype=jnp.int32
    )
    target = flat_ids * capacity + slot_rank
    token_of = jnp.arange(flat_ids.shape[0], dtype=jnp.int32) // top_count
    slot_token = jnp.zeros((expert_count * capacity,), jnp.int32).at[target].set(token_of)
    outgoing = normed[slot_token].reshape(expert_count, capacity, feature_width)
    arrived = lax.all_to_all(outgoing, ("ep", "tp"), split_axis=0, concat_axis=0, tiled=True)
    flat_in = arrived.reshape(expert_count * capacity, feature_width)
    gate_value = jnp.dot(flat_in, expert_gate[0], preferred_element_type=jnp.float32)
    up_value = jnp.dot(flat_in, expert_up[0], preferred_element_type=jnp.float32)
    active = (jax.nn.silu(gate_value) * up_value).astype(jnp.bfloat16)
    result = jnp.dot(active, expert_down[0], preferred_element_type=jnp.float32).astype(
        jnp.bfloat16
    )
    returned = lax.all_to_all(
        result.reshape(expert_count, capacity, feature_width),
        ("ep", "tp"),
        split_axis=0,
        concat_axis=0,
        tiled=True,
    )
    picked = returned.reshape(expert_count * capacity, feature_width)[target].astype(jnp.float32)
    weights = route_weights.reshape(-1)
    routed = jnp.sum(
        (weights[:, None] * picked).reshape(row_count, top_count, feature_width), axis=1
    )
    expert_rows = (shared_out + routed).astype(jnp.bfloat16)
    return (mixed_rows, expert_rows)


MESH = pl.DeviceIdType.MESH
BF = jnp.bfloat16
F32 = jnp.float32
CHUNKS = 2
PARTS = 4
PIECES = (CHUNKS,) + tuple(range(CHUNKS))


def dot(a, b):
    return jnp.dot(a, b, preferred_element_type=F32)


def fused_kernel(
    ep, tp,
    og_h, ig_h, iv_h, taps, mo_h, mgain, tok_h, egain, ids, wts, eg_h, eu_h, ed_h, sg_h, su_h, sd_h,
    mixed_ref, rows_ref,
    og, ig, iv, mo, tok, eg, eu, ed, sgu, halo, pbuf, scaled,
    gat, tab, act, dd, rc, rx, zd, zu, mp, mrc, mrx,
    load_sem, halo_sem, gz_r, gz_su, gz_sd, gx_r, gx_s, gc_r, gc_s,
    rc_r, rc_s, rx_r, rx_s, zd_r, zd_s, zu_r, zu_s, m_r, m_s,
):
    z = lax.axis_index("ep")
    t = lax.axis_index("tp")
    g = lax.axis_index("grp")
    x = t // 2
    c = t % 2
    rows = tok.shape[0]
    width = tok.shape[1]
    columns = ig.shape[1]
    sub = rows // CHUNKS
    up = (g, z + 1, t)
    down = (g, z - 1, t)
    xn = (g, z, (1 - x) * 2 + c)
    pc = (g, z, x * 2 + 1 - c)
    has_up = z < ep - 1
    has_down = z > 0

    loads = {}

    def load(name, src, dst):
        copy = pltpu.make_async_copy(src, dst, load_sem.at[len(loads)])
        copy.start()
        loads[name] = copy

    half = sd_h.shape[0]
    hid = eg.shape[1]
    load("tok", tok_h, tok)
    load("ig", ig_h, ig)
    load("iv", iv_h, iv)
    load("og", og_h, og)
    load("mo", mo_h, mo)
    load("sg", sg_h, sgu.at[:, pl.ds(0, half)])
    load("su", su_h, sgu.at[:, pl.ds(half, half)])
    load("sd", sd_h, ed.at[pl.ds(hid, half), :])
    load("eg", eg_h.at[0], eg)
    load("eu", eu_h.at[0], eu)
    load("ed", ed_h.at[0], ed.at[pl.ds(0, hid), :])

    barrier = pltpu.get_barrier_semaphore()
    for peer in (xn, pc):
        pl.semaphore_signal(barrier, inc=1, device_id=peer, device_id_type=MESH)

    @pl.when(has_up)
    def _():
        pl.semaphore_signal(barrier, inc=1, device_id=up, device_id_type=MESH)

    @pl.when(has_down)
    def _():
        pl.semaphore_signal(barrier, inc=1, device_id=down, device_id_type=MESH)

    def rcopy(src, dst, ssem, rsem, peer):
        return pltpu.make_async_remote_copy(
            src_ref=src, dst_ref=dst, send_sem=ssem, recv_sem=rsem, device_id=peer, device_id_type=MESH
        )

    def block(zz, xx, cc):
        return (zz * 2 + xx) * 2 + cc

    def piece(zz, xx, cc, k):
        if k == CHUNKS:
            return tab.at[block(zz, xx, cc)]
        return gat.at[pl.ds(pl.multiple_of(block(zz, xx, cc) * rows + k * sub, sub), sub), :]

    def whole(zz, xx, cc):
        return gat.at[pl.ds(pl.multiple_of(block(zz, xx, cc) * rows, rows), rows), :]

    def c_up(zz, k):
        return rcopy(piece(zz, x, c, k), piece(zz, x, c, k), gz_su.at[zz, k], gz_r.at[zz, k], up)

    def c_down(zz, k):
        return rcopy(piece(zz, x, c, k), piece(zz, x, c, k), gz_sd.at[zz, k], gz_r.at[zz, k], down)

    def c_x(zz, k):
        return rcopy(piece(zz, x, c, k), piece(zz, x, c, k), gx_s.at[zz, k], gx_r.at[zz, k], xn)

    def x_arrival(zz, k):
        return rcopy(piece(zz, 1 - x, c, k), piece(zz, 1 - x, c, k), gx_s.at[zz, k], gx_r.at[zz, k], xn)

    def core_pair(zz, xx, cc):
        names = tab.at[block(zz, xx, cc)]
        return (
            rcopy(whole(zz, xx, cc), whole(zz, xx, cc), gc_s.at[zz, xx, 0], gc_r.at[zz, xx, 0], pc),
            rcopy(names, names, gc_s.at[zz, xx, 1], gc_r.at[zz, xx, 1], pc),
        )

    def core_start(zz, xx):
        for copy in core_pair(zz, xx, c):
            copy.start()

    loads["tok"].wait()
    name_i = lax.broadcasted_iota(jnp.int32, (tab.shape[1], rows), 0)
    table = jnp.zeros((tab.shape[1], rows), F32)
    for k in range(ids.shape[0]):
        table = table + jnp.where(ids[k : k + 1, :] == name_i, wts[k : k + 1, :], 0.0)
    tab[block(z, x, c)] = jnp.zeros(tab.shape[1:], BF)
    tab[block(z, x, c), :, :rows] = table.astype(BF)
    v = tok[...].astype(F32)
    v = v * lax.rsqrt(jnp.mean(v * v, axis=-1, keepdims=True) + EPSILON) * egain[...]
    own = pl.ds(pl.multiple_of(block(z, x, c) * rows, rows), rows)
    gat[own, :] = v.astype(BF)

    pl.semaphore_wait(barrier, 2 + jnp.minimum(z, 1) + jnp.minimum(ep - 1 - z, 1))

    for k in PIECES:
        @pl.when(has_up)
        def _():
            c_up(z, k).start()

        @pl.when(has_down)
        def _():
            c_down(z, k).start()

        c_x(z, k).start()
    core_start(z, x)

    loads["ig"].wait()
    loads["iv"].wait()
    tail = ig.shape[0] - halo.shape[1]
    edge = halo.shape[1]
    h_gate = rcopy(ig.at[pl.ds(tail, edge)], halo.at[0], halo_sem.at[0], halo_sem.at[1], up)
    h_value = rcopy(iv.at[pl.ds(tail, edge)], halo.at[1], halo_sem.at[2], halo_sem.at[3], up)

    @pl.when(has_up)
    def _():
        h_gate.start()
        h_value.start()

    count = ig.shape[0]
    tile = width // 4

    def cols(n):
        return pl.ds(pl.multiple_of(n * tile, tile), tile)

    def m_core(xx):
        return rcopy(mp.at[xx * 2 + 1 - c], mrc.at[xx], m_s.at[xx], m_r.at[xx], pc)

    def mixer():
        pbuf[8:, :] = ig[...].astype(F32) * iv[...].astype(F32)

        @pl.when(jnp.logical_not(has_down))
        def _():
            pbuf[:8, :] = jnp.zeros((8, columns), F32)

        @pl.when(has_down)
        def _():
            h_gate.wait_recv()
            h_value.wait_recv()
            pbuf[:8, :] = halo[0, edge - 8 :, :].astype(F32) * halo[1, edge - 8 :, :].astype(F32)

        loads["og"].wait()
        tap = taps[:, pl.ds(pl.multiple_of(t * columns, columns), columns)].astype(F32)
        filtered = (
            tap[0:1] * pbuf[6 : 6 + count, :] + tap[1:2] * pbuf[7 : 7 + count, :] + tap[2:3] * pbuf[8 : 8 + count, :]
        )
        scaled[...] = (og[...].astype(F32) * filtered).astype(BF)
        loads["mo"].wait()
        @pl.loop(0, 4)
        def _(n):
            part = dot(scaled[...], mo[:, cols(n)]).astype(BF)
            mp[:, :, cols(n)] = part.reshape(tp, rows, tile)

        for xx in range(2):
            m_core(xx).start()

    def z_step(s):
        for k in PIECES:
            @pl.when(z >= s)
            def _():
                c_up(z - s, k).wait_recv()

                @pl.when(has_up)
                def _():
                    c_up(z - s, k).start()

                c_x(z - s, k).start()

            @pl.when(z + s < ep)
            def _():
                c_down(z + s, k).wait_recv()

                @pl.when(has_down)
                def _():
                    c_down(z + s, k).start()

                c_x(z + s, k).start()

        @pl.when(z >= s)
        def _():
            core_start(z - s, x)

        @pl.when(z + s < ep)
        def _():
            core_start(z + s, x)

    def x_step(zz):
        for k in PIECES:
            x_arrival(zz, k).wait_recv()
        core_start(zz, 1 - x)

    def core_step(zz):
        for xx in range(2):
            for copy in core_pair(zz, xx, 1 - c):
                copy.wait_recv()

    def nth(n):
        near = jnp.minimum(z, ep - 1 - z)
        d = (n + 1) // 2
        side = z - d if n % 2 else z + d
        far = jnp.where(z < ep - 1 - z, n, ep - 1 - n)
        return jnp.where(n <= 2 * near, side, far)

    order = [nth(n) for n in range(ep)]

    def group(zz):
        return pl.ds(pl.multiple_of(zz * tp * rows, tp * rows), tp * rows)

    tokens = tp * rows
    expert = z * tp + t
    picked = lax.broadcasted_iota(jnp.int32, (tab.shape[1], tab.shape[2]), 0) == expert
    diagonal = lax.broadcasted_iota(jnp.int32, (rows, tab.shape[2]), 0) == lax.broadcasted_iota(
        jnp.int32, (rows, tab.shape[2]), 1
    )

    def weight_column(block_id):
        line = jnp.sum(jnp.where(picked, tab[block_id].astype(F32), 0.0), axis=0, keepdims=True)
        return jnp.sum(jnp.where(diagonal, line, 0.0), axis=1, keepdims=True)

    def shared():
        for name in ("sg", "su", "sd"):
            loads[name].wait()
        hidden = dot(gat[group(z), :], sgu[...])
        gate, value = hidden[:, :half], hidden[:, half:]
        act[:, hid:] = (gate / (1.0 + jnp.exp(-gate)) * value).astype(BF)

    def experts(zz, depth):
        weight = jnp.concatenate([weight_column(zz * tp + i) for i in range(tp)], axis=0)
        step = 256 if hid % 256 == 0 else hid

        @pl.loop(0, hid // step)
        def _(n):
            col = pl.ds(pl.multiple_of(n * step, step), step)
            gate = dot(gat[group(zz), :], eg[:, col])
            value = dot(gat[group(zz), :], eu[:, col])
            act[:, col] = (gate / (1.0 + jnp.exp(-gate)) * value * weight).astype(BF)

        @pl.loop(0, 4)
        def _(n):
            out = dot(act[:, :depth], ed[:depth, cols(n)])
            dst = pl.ds(pl.multiple_of(zz * tp, tp), tp)
            dd[dst, :, cols(n)] = out.astype(BF).reshape(tp, rows, tile)

    def d_core(zz, xx):
        return rcopy(dd.at[block(zz, xx, 1 - c)], rc.at[zz, xx], rc_s.at[zz, xx], rc_r.at[zz, xx], pc)

    deep = rows // PARTS

    def part_of(ref, p):
        return ref.at[pl.ds(p * deep, deep)]

    def d_x(zz, p):
        src = part_of(dd.at[block(zz, 1 - x, c)], p)
        return rcopy(src, part_of(rx.at[zz], p), rx_s.at[zz, p], rx_r.at[zz, p], xn)

    def d_up(zz, p):
        src = part_of(dd.at[block(zz, x, c)], p)
        return rcopy(src, part_of(zu.at[zz], p), zu_s.at[zz, p], zu_r.at[zz, p], up)

    def d_down(zz, p):
        src = part_of(dd.at[block(zz, x, c)], p)
        return rcopy(src, part_of(zd.at[zz], p), zd_s.at[zz, p], zd_r.at[zz, p], down)

    def compute(zz, depth):
        core_step(zz)
        experts(zz, depth)
        for xx in range(2):
            d_core(zz, xx).start()

    def fold_core(zz):
        for xx in range(2):
            d_core(zz, xx).wait_recv()
        there = block(zz, 1 - x, c)
        dd[there] = (dd[there].astype(F32) + rc[zz, 1 - x].astype(F32)).astype(BF)
        for p in range(PARTS):
            d_x(zz, p).start()

    def fold_z(zz):
        here = block(zz, x, c)
        lower = zz < z
        for p in range(PARTS):
            band = pl.ds(p * deep, deep)
            d_x(zz, p).wait_recv()
            so_far = (
                dd[here, band].astype(F32) + rc[zz, x, band].astype(F32) + rx[zz, band].astype(F32)
            )

            @pl.when(jnp.logical_and(lower, has_up))
            def _():
                d_down(zz, p).wait_recv()
                dd[here, band] = (so_far + zd[zz, band].astype(F32)).astype(BF)

            @pl.when(jnp.logical_and(jnp.logical_not(lower), has_down))
            def _():
                d_up(zz, p).wait_recv()
                dd[here, band] = (so_far + zu[zz, band].astype(F32)).astype(BF)

            @pl.when(jnp.where(lower, jnp.logical_not(has_up), jnp.logical_not(has_down)))
            def _():
                dd[here, band] = so_far.astype(BF)

            @pl.when(lower)
            def _():
                d_down(zz, p).start()

            @pl.when(jnp.logical_not(lower))
            def _():
                d_up(zz, p).start()

    lower_half = 2 * z < ep

    def target(n):
        found = 0
        for edge in range((ep + 1) // 2):
            ranked = sorted((l for l in range(ep) if l != edge), key=lambda l: (-abs(l - edge), l))
            found = jnp.where(jnp.minimum(z, ep - 1 - z) == edge, ranked[n - 1], found)
        return jnp.where(lower_half, found, ep - 1 - found)

    m_x = rcopy(mp.at[(1 - x) * 2 + c], mrx, m_s.at[2], m_r.at[2], xn)

    def mixer_send():
        for xx in range(2):
            m_core(xx).wait_recv()
        mine = (1 - x) * 2 + c
        mp[mine] = (mp[mine].astype(F32) + mrc[1 - x].astype(F32)).astype(BF)
        m_x.start()

    z_step(1)
    x_step(order[0])
    if ep > 2:
        z_step(2)
    core_step(order[0])
    shared()
    for name in ("eg", "eu", "ed"):
        loads[name].wait()
    experts(order[0], hid + half)
    for xx in range(2):
        d_core(order[0], xx).start()
    x_step(order[1])
    mixer()
    for s in range(3, ep):
        z_step(s)
    for n in range(2, ep):
        x_step(order[n])
    for n in range(1, ep - 1):
        compute(order[n], hid)
        if n == 1:
            fold_core(order[1])
    compute(order[ep - 1], hid)
    for n in range(ep - 1, 1 if ep > 2 else 0, -1):
        fold_core(order[n])
    mixer_send()
    fold_core(order[0])
    for n in range(1, ep):
        fold_z(target(n))

    m_x.wait_recv()
    mixed = mp[t].astype(F32) + mrc[x].astype(F32) + mrx[...].astype(F32)
    scale = lax.rsqrt(jnp.mean(mixed * mixed, axis=-1, keepdims=True) + EPSILON)
    mixed_ref[...] = (mixed * scale * mgain[...]).astype(BF)

    here = block(z, x, c)
    for p in range(PARTS):
        band = pl.ds(p * deep, deep)
        d_x(z, p).wait_recv()
        total = dd[here, band].astype(F32) + rc[z, x, band].astype(F32) + rx[z, band].astype(F32)

        @pl.when(jnp.logical_not(has_up))
        def _():
            d_up(z, p).wait_recv()
            rows_ref[band, :] = (total + zu[z, band].astype(F32)).astype(BF)

        @pl.when(jnp.logical_not(has_down))
        def _():
            d_down(z, p).wait_recv()
            rows_ref[band, :] = (total + zd[z, band].astype(F32)).astype(BF)

        @pl.when(jnp.logical_and(has_up, has_down))
        def _():
            d_up(z, p).wait_recv()
            d_down(z, p).wait_recv()
            rows_ref[band, :] = (
                total + zu[z, band].astype(F32) + zd[z, band].astype(F32)
            ).astype(BF)

    @pl.when(has_up)
    def _():
        h_gate.wait_send()
        h_value.wait_send()

    for zz in range(ep):
        @pl.when(jnp.logical_and(has_up, zz <= z))
        def _():
            for k in PIECES:
                c_up(zz, k).wait_send()

        @pl.when(jnp.logical_and(has_down, zz >= z))
        def _():
            for k in PIECES:
                c_down(zz, k).wait_send()

        for k in PIECES:
            c_x(zz, k).wait_send()
        for xx in range(2):
            for copy in core_pair(zz, xx, c):
                copy.wait_send()
            d_core(zz, xx).wait_send()
        for p in range(PARTS):
            d_x(zz, p).wait_send()

        @pl.when(zz < z)
        def _():
            for p in range(PARTS):
                d_down(zz, p).wait_send()

        @pl.when(zz > z)
        def _():
            for p in range(PARTS):
                d_up(zz, p).wait_send()

    for xx in range(2):
        m_core(xx).wait_send()
    m_x.wait_send()


def fused_on_device(ep, tp, *args):
    (og, ig, iv, taps, mo, mgain, tok, egain, ids, wts, eg, eu, ed, sg, su, sd) = args
    rows, width = tok.shape
    count, columns = ig.shape
    experts = ep * tp
    names = -(-experts // 16) * 16
    hid = eg.shape[2]
    half = sd.shape[0]
    any_spec = pl.BlockSpec(memory_space=pltpu.HBM)
    vmem = pl.BlockSpec(memory_space=pltpu.VMEM)
    dma = pltpu.SemaphoreType.DMA
    V = pltpu.VMEM
    return pl.pallas_call(
        functools.partial(fused_kernel, ep, tp),
        out_shape=(V((rows, width), BF), V((rows, width), BF)),
        in_specs=[any_spec] * 3 + [vmem, any_spec, vmem, any_spec, vmem, vmem, vmem] + [any_spec] * 6,
        out_specs=(vmem, vmem),
        scratch_shapes=[
            V((count, columns), BF), V((count, columns), BF), V((count, columns), BF),
            V((columns, width), BF), V((rows, width), BF),
            V((width, hid), BF), V((width, hid), BF), V((hid + half, width), BF),
            V((width, 2 * half), BF),
            V((2, 16, columns), BF), V((count + 8, columns), F32), V((count, columns), BF),
            V((experts * rows, width), BF), V((experts, names, 128), BF),
            V((tp * rows, hid + half), BF),
            V((experts, rows, width), BF), V((ep, 2, rows, width), BF), V((ep, rows, width), BF),
            V((ep, rows, width), BF), V((ep, rows, width), BF),
            V((tp, rows, width), BF), V((2, rows, width), BF), V((rows, width), BF),
            dma((11,)), dma((4,)),
            dma((ep, CHUNKS + 1)), dma((ep, CHUNKS + 1)), dma((ep, CHUNKS + 1)),
            dma((ep, CHUNKS + 1)), dma((ep, CHUNKS + 1)), dma((ep, 2, 2)), dma((ep, 2, 2)),
            dma((ep, 2)), dma((ep, 2)), dma((ep, PARTS)), dma((ep, PARTS)),
            dma((ep, PARTS)), dma((ep, PARTS)), dma((ep, PARTS)), dma((ep, PARTS)), dma((3,)), dma((3,)),
        ],
        compiler_params=pltpu.CompilerParams(
            collective_id=0, has_side_effects=True, vmem_limit_bytes=60 * 1024 * 1024
        ),
    )(
        og, ig, iv, taps, mo, mgain.reshape(1, -1), tok, egain.reshape(1, -1), ids.T, wts.T, eg, eu, ed, sg, su, sd
    )


def plan(mesh):
    ep, tp = mesh.shape["ep"], mesh.shape["tp"]
    if tp == 4 and ep % 2 == 0 and ep <= 4:
        return functools.partial(fused_on_device, ep, tp)
    return on_device


def solution(mesh):
    return jax.shard_map(
        plan(mesh),
        mesh=mesh,
        in_specs=(
            P(("grp", "ep"), "tp"),
            P(("grp", "ep"), "tp"),
            P(("grp", "ep"), "tp"),
            P(),
            P("tp", None),
            P(),
            P(("grp", "ep", "tp"), None),
            P(),
            P(("grp", "ep", "tp"), None),
            P(("grp", "ep", "tp"), None),
            P(("ep", "tp"), None, None),
            P(("ep", "tp"), None, None),
            P(("ep", "tp"), None, None),
            P(None, "tp"),
            P(None, "tp"),
            P("tp", None),
        ),
        out_specs=(P(("grp", "ep", "tp"), None), P(("grp", "ep", "tp"), None)),
        check_vma=False,
    )
```

```python
import functools
import jax
import jax.numpy as jnp
from jax import lax
from jax.experimental import pallas as pl
from jax.experimental.pallas import tpu as pltpu
from jax.sharding import PartitionSpec as P

EPSILON = 1e-06


def passed_along(array, axis, by):
    size = lax.axis_size(axis)
    pairs = [(i, i + by) for i in range(size) if 0 <= i + by < size]
    return lax.ppermute(array, axis, pairs)


def rms_scale(values, gains):
    return values * lax.rsqrt(jnp.mean(values * values, axis=-1, keepdims=True) + EPSILON) * gains


def on_device(
    outer_gate,
    inner_gate,
    inner_value,
    conv_taps,
    mixer_out,
    mixer_gain,
    moe_tokens,
    expert_gain,
    route_ids,
    route_weights,
    expert_gate,
    expert_up,
    expert_down,
    shared_gate,
    shared_up,
    shared_down,
):
    columns = inner_gate.shape[1]
    kernel = lax.dynamic_slice_in_dim(conv_taps, lax.axis_index("tp") * columns, columns, 1).astype(
        jnp.float32
    )
    before_gate, before_value = passed_along((inner_gate[-2:], inner_value[-2:]), "ep", 1)
    gate_rows = jnp.concatenate([before_gate, inner_gate], axis=0).astype(jnp.float32)
    value_rows = jnp.concatenate([before_value, inner_value], axis=0).astype(jnp.float32)
    product = gate_rows * value_rows
    filtered = kernel[0] * product[:-2] + kernel[1] * product[1:-1] + kernel[2] * product[2:]
    scaled = (outer_gate.astype(jnp.float32) * filtered).astype(jnp.bfloat16)
    normed = rms_scale(moe_tokens.astype(jnp.float32), expert_gain).astype(jnp.bfloat16)
    feature_width = normed.shape[1]
    piece = lax.all_gather(normed, "tp", axis=0, tiled=True)
    gate_value = jnp.dot(piece, shared_gate, preferred_element_type=jnp.float32)
    up_value = jnp.dot(piece, shared_up, preferred_element_type=jnp.float32)
    shared_act = (jax.nn.silu(gate_value) * up_value).astype(jnp.bfloat16)
    mixer_part = jnp.dot(scaled, mixer_out, preferred_element_type=jnp.float32)
    shared_part = jnp.dot(shared_act, shared_down, preferred_element_type=jnp.float32)
    both_sums = lax.psum_scatter(
        jnp.concatenate([mixer_part, shared_part], axis=1).astype(jnp.bfloat16),
        "tp",
        scatter_dimension=0,
        tiled=True,
    ).astype(jnp.float32)
    mixed_rows = rms_scale(both_sums[:, :feature_width], mixer_gain).astype(jnp.bfloat16)
    shared_out = both_sums[:, feature_width:]
    row_count, top_count = route_ids.shape
    ep_count = lax.axis_size("ep")
    tp_count = lax.axis_size("tp")
    expert_count = ep_count * tp_count
    capacity = (3 * row_count * top_count + 2 * expert_count - 1) // (2 * expert_count)
    flat_ids = route_ids.reshape(-1)
    onehot = (flat_ids[:, None] == jnp.arange(expert_count, dtype=jnp.int32)[None, :]).astype(
        jnp.int32
    )
    slot_rank = jnp.sum(
        (jnp.cumsum(onehot, axis=0, dtype=jnp.int32) - onehot) * onehot, axis=1, dtype=jnp.int32
    )
    target = flat_ids * capacity + slot_rank
    token_of = jnp.arange(flat_ids.shape[0], dtype=jnp.int32) // top_count
    slot_token = jnp.zeros((expert_count * capacity,), jnp.int32).at[target].set(token_of)
    outgoing = normed[slot_token].reshape(expert_count, capacity, feature_width)
    arrived = lax.all_to_all(outgoing, ("ep", "tp"), split_axis=0, concat_axis=0, tiled=True)
    flat_in = arrived.reshape(expert_count * capacity, feature_width)
    gate_value = jnp.dot(flat_in, expert_gate[0], preferred_element_type=jnp.float32)
    up_value = jnp.dot(flat_in, expert_up[0], preferred_element_type=jnp.float32)
    active = (jax.nn.silu(gate_value) * up_value).astype(jnp.bfloat16)
    result = jnp.dot(active, expert_down[0], preferred_element_type=jnp.float32).astype(
        jnp.bfloat16
    )
    returned = lax.all_to_all(
        result.reshape(expert_count, capacity, feature_width),
        ("ep", "tp"),
        split_axis=0,
        concat_axis=0,
        tiled=True,
    )
    picked = returned.reshape(expert_count * capacity, feature_width)[target].astype(jnp.float32)
    weights = route_weights.reshape(-1)
    routed = jnp.sum(
        (weights[:, None] * picked).reshape(row_count, top_count, feature_width), axis=1
    )
    expert_rows = (shared_out + routed).astype(jnp.bfloat16)
    return (mixed_rows, expert_rows)


MESH = pl.DeviceIdType.MESH
BF = jnp.bfloat16
F32 = jnp.float32
CHUNKS = 2
PARTS = 4
HALVES = 2
PIECES = (CHUNKS,) + tuple(range(CHUNKS))


def dot(a, b):
    return jnp.dot(a, b, preferred_element_type=F32)


def dot_rows(a, b):
    return lax.dot_general(a, b, (((0,), (0,)), ((), ())), preferred_element_type=F32)


def fused_kernel(
    ep, tp, cap, slot,
    og_h, ig_h, iv_h, taps, mo_h, mgain, tok_h, egain, ids, wts, eg_h, eu_h, ed_h, sg_h, su_h, sd_h,
    mixed_ref, rows_ref,
    og, ig, iv, mo, tok, eg, eu, ed, sgu, halo, pbuf, scaled,
    gat, tab, act, dd, packed, spread, rc, back, rx, edge_in, last_in, mp, mrc, mrx,
    load_sem, halo_sem, gz_r, gz_su, gz_sd, gx_r, gx_s, gc_r, gc_s, px_r, px_s,
    rc_r, rc_s, q_r, q_s, rx_r, rx_s, e_r, e_s, f_r, f_s, m_r, m_s,
):
    z = lax.axis_index("ep")
    t = lax.axis_index("tp")
    g = lax.axis_index("grp")
    x = t // 2
    c = t % 2
    rows = tok.shape[0]
    width = tok.shape[1]
    columns = ig.shape[1]
    sub = rows // CHUNKS
    up = (g, z + 1, t)
    down = (g, z - 1, t)
    xn = (g, z, (1 - x) * 2 + c)
    pc = (g, z, x * 2 + 1 - c)
    xd = (g, z, (1 - x) * 2 + 1 - c)
    z2 = (g, (z + 2) % ep, t)
    is_edge = jnp.logical_or(z == 0, z == ep - 1)
    inner = jnp.where(2 * z < ep, z + 1, z - 1)
    outer = jnp.where(2 * z < ep, z - 1, z + 1)
    has_up = z < ep - 1
    has_down = z > 0

    loads = {}

    def load(name, src, dst):
        copy = pltpu.make_async_copy(src, dst, load_sem.at[len(loads)])
        copy.start()
        loads[name] = copy

    half = sd_h.shape[0]
    hid = eg.shape[1]
    load("tok", tok_h, tok)
    load("ig", ig_h, ig)
    load("iv", iv_h, iv)
    load("og", og_h, og)
    load("mo", mo_h, mo)
    load("sg", sg_h, sgu.at[:, pl.ds(0, half)])
    load("su", su_h, sgu.at[:, pl.ds(half, half)])
    load("sd", sd_h, ed.at[pl.ds(hid, half), :])
    load("eg", eg_h.at[0], eg)
    load("eu", eu_h.at[0], eu)
    load("ed", ed_h.at[0], ed.at[pl.ds(0, hid), :])

    barrier = pltpu.get_barrier_semaphore()
    for peer in (xn, pc, xd, z2):
        pl.semaphore_signal(barrier, inc=1, device_id=peer, device_id_type=MESH)

    @pl.when(has_up)
    def _():
        pl.semaphore_signal(barrier, inc=1, device_id=up, device_id_type=MESH)

    @pl.when(has_down)
    def _():
        pl.semaphore_signal(barrier, inc=1, device_id=down, device_id_type=MESH)

    def rcopy(src, dst, ssem, rsem, peer):
        return pltpu.make_async_remote_copy(
            src_ref=src, dst_ref=dst, send_sem=ssem, recv_sem=rsem, device_id=peer, device_id_type=MESH
        )

    def block(zz, side, cc):
        return (zz * 2 + side) * 2 + cc

    def lines(zz, side, cc):
        return pl.ds(pl.multiple_of(block(zz, side, cc) * rows, rows), rows)

    def few(zz, cc):
        return pl.ds(pl.multiple_of(block(zz, 1, 0) * rows + cc * slot, slot), cap)

    def slots_of(cc):
        return pl.ds(pl.multiple_of(cc * slot, slot), cap)

    def piece(zz, side, cc, k):
        if k == CHUNKS:
            return tab.at[block(zz, side, cc)]
        return gat.at[pl.ds(pl.multiple_of(block(zz, side, cc) * rows + k * sub, sub), sub), :]

    def c_up(zz, k):
        return rcopy(piece(zz, 0, c, k), piece(zz, 0, c, k), gz_su.at[zz, k], gz_r.at[zz, k], up)

    def c_down(zz, k):
        return rcopy(piece(zz, 0, c, k), piece(zz, 0, c, k), gz_sd.at[zz, k], gz_r.at[zz, k], down)

    def c_x(k):
        return rcopy(piece(z, 0, c, k), piece(z, 1, c, k), gx_s.at[k], gx_r.at[k], xn)

    def core_pair(zz, side, cc):
        names = tab.at[block(zz, side, cc)]
        body = gat.at[lines(zz, side, cc), :]
        return (
            rcopy(body, body, gc_s.at[zz, side, 0], gc_r.at[zz, side, 0], pc),
            rcopy(names, names, gc_s.at[zz, side, 1], gc_r.at[zz, side, 1], pc),
        )

    def core_start(zz, side):
        for copy in core_pair(zz, side, c):
            copy.start()

    def few_pair(zz):
        return (
            rcopy(packed.at[zz, slots_of(c), :], gat.at[few(zz, c), :], px_s.at[zz, 0], px_r.at[zz, 0], xn),
            rcopy(packed.at[zz, slots_of(1 - c), :], gat.at[few(zz, c), :], px_s.at[zz, 1], px_r.at[zz, 1], xd),
        )

    for zz in range(ep):
        for e in range(2):
            back[zz, pl.ds(e * slot + cap, slot - cap), :] = jnp.zeros((slot - cap, width), BF)

    loads["tok"].wait()
    name_i = lax.broadcasted_iota(jnp.int32, (tab.shape[1], rows), 0)
    table = jnp.zeros((tab.shape[1], rows), F32)
    for k in range(ids.shape[0]):
        table = table + jnp.where(ids[k : k + 1, :] == name_i, wts[k : k + 1, :], 0.0)
    tab[block(z, 0, c)] = jnp.zeros(tab.shape[1:], BF)
    tab[block(z, 0, c), :, :rows] = table.astype(BF)
    v = tok[...].astype(F32)
    v = v * lax.rsqrt(jnp.mean(v * v, axis=-1, keepdims=True) + EPSILON) * egain[...]
    gat[lines(z, 0, c), :] = v.astype(BF)

    pl.semaphore_wait(barrier, 4 + jnp.minimum(z, 1) + jnp.minimum(ep - 1 - z, 1))

    loads["ig"].wait()
    loads["iv"].wait()
    tail = ig.shape[0] - halo.shape[1]
    edge = halo.shape[1]
    h_gate = rcopy(ig.at[pl.ds(tail, edge)], halo.at[0], halo_sem.at[0], halo_sem.at[1], up)
    h_value = rcopy(iv.at[pl.ds(tail, edge)], halo.at[1], halo_sem.at[2], halo_sem.at[3], up)

    @pl.when(has_up)
    def _():
        h_gate.start()
        h_value.start()

    for k in PIECES:
        @pl.when(has_up)
        def _():
            c_up(z, k).start()

        @pl.when(has_down)
        def _():
            c_down(z, k).start()

        c_x(k).start()
    core_start(z, 0)

    count = ig.shape[0]
    tile = width // PARTS

    def cols(n):
        return pl.ds(pl.multiple_of(n * tile, tile), tile)

    def m_core(xx):
        return rcopy(mp.at[xx * 2 + 1 - c], mrc.at[xx], m_s.at[xx], m_r.at[xx], pc)

    def mixer():
        pbuf[8:, :] = ig[...].astype(F32) * iv[...].astype(F32)

        @pl.when(jnp.logical_not(has_down))
        def _():
            pbuf[:8, :] = jnp.zeros((8, columns), F32)

        @pl.when(has_down)
        def _():
            h_gate.wait_recv()
            h_value.wait_recv()
            pbuf[:8, :] = halo[0, edge - 8 :, :].astype(F32) * halo[1, edge - 8 :, :].astype(F32)

        loads["og"].wait()
        tap = taps[:, pl.ds(pl.multiple_of(t * columns, columns), columns)].astype(F32)
        filtered = (
            tap[0:1] * pbuf[6 : 6 + count, :] + tap[1:2] * pbuf[7 : 7 + count, :] + tap[2:3] * pbuf[8 : 8 + count, :]
        )
        scaled[...] = (og[...].astype(F32) * filtered).astype(BF)
        loads["mo"].wait()
        @pl.loop(0, 4)
        def _(n):
            part = dot(scaled[...], mo[:, cols(n)]).astype(BF)
            mp[:, :, cols(n)] = part.reshape(tp, rows, tile)

        for xx in range(2):
            m_core(xx).start()

    lanes = tab.shape[2]
    name_of = lax.broadcasted_iota(jnp.int32, (tab.shape[1], lanes), 0)
    before = (
        lax.broadcasted_iota(jnp.int32, (lanes, lanes), 0) < lax.broadcasted_iota(jnp.int32, (lanes, lanes), 1)
    ).astype(BF)
    slot_i = lax.broadcasted_iota(jnp.int32, (slot, lanes), 0)
    diagonal = lax.broadcasted_iota(jnp.int32, (rows, lanes), 0) == lax.broadcasted_iota(
        jnp.int32, (rows, lanes), 1
    )
    expert = z * tp + t

    def line_of(name, block_id):
        return jnp.sum(jnp.where(name_of == name, tab[block_id].astype(F32), 0.0), axis=0, keepdims=True)

    def weight_column(block_id):
        return jnp.sum(jnp.where(diagonal, line_of(expert, block_id), 0.0), axis=1, keepdims=True)

    def compact(zz):
        marks = []
        for e in range(2):
            weight = line_of(z * tp + (1 - x) * 2 + e, block(zz, 0, c))
            named = weight > 0
            ahead = dot(jnp.broadcast_to(named, (8, lanes)).astype(F32).astype(BF), before)[0:1]
            hit = jnp.logical_and(slot_i == ahead.astype(jnp.int32), named)
            marks.append(hit.astype(F32))
            spread[zz, pl.ds(e * slot, slot), :] = jnp.where(hit, weight, 0.0).astype(BF)
        mark = jnp.concatenate(marks, axis=0).astype(BF)[:, :rows]

        @pl.loop(0, PARTS)
        def _(n):
            packed[zz, :, cols(n)] = dot(mark, gat[lines(zz, 0, c), cols(n)]).astype(BF)

        for copy in few_pair(zz):
            copy.start()

    def z_step(s):
        for k in PIECES:
            @pl.when(z >= s)
            def _():
                c_up(z - s, k).wait_recv()

                @pl.when(has_up)
                def _():
                    c_up(z - s, k).start()

            @pl.when(z + s < ep)
            def _():
                c_down(z + s, k).wait_recv()

                @pl.when(has_down)
                def _():
                    c_down(z + s, k).start()

        @pl.when(z >= s)
        def _():
            core_start(z - s, 0)

        @pl.when(z + s < ep)
        def _():
            core_start(z + s, 0)

    def compacts(s):
        @pl.when(z >= s)
        def _():
            compact(z - s)

        @pl.when(z + s < ep)
        def _():
            compact(z + s)

    def own_x():
        for k in PIECES:
            c_x(k).wait_recv()
        core_start(z, 1)

    def core_step(zz, sides):
        for side in range(sides):
            for copy in core_pair(zz, side, 1 - c):
                copy.wait_recv()
        if sides == 1:
            for copy in few_pair(zz):
                copy.wait_recv()

    def nth(n):
        near = jnp.minimum(z, ep - 1 - z)
        d = (n + 1) // 2
        side = z - d if n % 2 else z + d
        far = jnp.where(z < ep - 1 - z, n, ep - 1 - n)
        return jnp.where(n <= 2 * near, side, far)

    order = [nth(n) for n in range(ep)]

    def shared():
        for name in ("sg", "su", "sd"):
            loads[name].wait()
        own = pl.ds(pl.multiple_of(block(z, 0, 0) * rows, tp * rows), tp * rows)
        hidden = dot(gat[own, :], sgu[...])
        gate, value = hidden[:, :half], hidden[:, half:]
        act[:, hid:] = (gate / (1.0 + jnp.exp(-gate)) * value).astype(BF)

    def experts(zz, sides):
        depth = hid + half if sides == 2 else hid
        weights = [weight_column(block(zz, side, cc)) for side in range(sides) for cc in range(2)]
        if sides == 1:
            weights.append(jnp.ones((2 * slot, 1), F32))
        weight = jnp.concatenate(weights, axis=0)
        amount = weight.shape[0]
        span = pl.ds(pl.multiple_of(block(zz, 0, 0) * rows, tp * rows), amount)
        step = 256 if hid % 256 == 0 else hid

        @pl.loop(0, hid // step)
        def _(n):
            col = pl.ds(pl.multiple_of(n * step, step), step)
            gate = dot(gat[span, :], eg[:, col])
            value = dot(gat[span, :], eu[:, col])
            act[:amount, col] = (gate / (1.0 + jnp.exp(-gate)) * value * weight).astype(BF)

        @pl.loop(0, PARTS)
        def _(n):
            dd[span, cols(n)] = dot(act[:amount, :depth], ed[:depth, cols(n)]).astype(BF)

    def d_core(zz, side):
        at = zz if side == 0 else ep
        return rcopy(dd.at[lines(zz, side, 1 - c), :], rc.at[at], rc_s.at[at], rc_r.at[at], pc)

    wide = width // HALVES

    def d_few(zz, h):
        part = pl.ds(h * wide, wide)
        return (
            rcopy(
                dd.at[few(zz, c), part], back.at[zz, slots_of(c), part],
                q_s.at[zz, h, 0], q_r.at[zz, h, 0], xn,
            ),
            rcopy(
                dd.at[few(zz, 1 - c), part], back.at[zz, slots_of(c), part],
                q_s.at[zz, h, 1], q_r.at[zz, h, 1], xd,
            ),
        )

    def d_x(p):
        return rcopy(dd.at[lines(z, 1, c), cols(p)], rx.at[:, cols(p)], rx_s.at[p], rx_r.at[p], xn)

    def to_inner(zz, p):
        src = dd.at[lines(zz, 0, c), cols(p)]
        return rcopy(src, edge_in.at[zz, :, cols(p)], e_s.at[zz, p], e_r.at[zz, p], (g, inner, t))

    def to_owner(zz, p):
        owner_is_edge = jnp.logical_or(zz == 0, zz == ep - 1)
        place = jnp.where(jnp.logical_and(owner_is_edge, zz == outer), 0, 1)
        src = dd.at[lines(zz, 0, c), cols(p)]
        return rcopy(src, last_in.at[place, :, cols(p)], f_s.at[zz, p], f_r.at[place, p], (g, zz, t))

    def last_arrival(place, p):
        here = last_in.at[place, :, cols(p)]
        return rcopy(here, here, f_s.at[place, p], f_r.at[place, p], xn)

    def compute(zz):
        core_step(zz, 1)
        experts(zz, 1)
        d_core(zz, 0).start()
        for h in range(HALVES):
            for copy in d_few(zz, h):
                copy.start()

    def fold_core():
        d_core(z, 1).wait_recv()
        there = lines(z, 1, c)
        dd[there, :] = (dd[there, :].astype(F32) + rc[ep].astype(F32)).astype(BF)
        for p in range(PARTS):
            d_x(p).start()

    def fold_z(zz):
        here = lines(zz, 0, c)
        d_core(zz, 0).wait_recv()
        for p in range(PARTS):
            band = cols(p)
            if p % (PARTS // HALVES) == 0:
                for copy in d_few(zz, p // (PARTS // HALVES)):
                    copy.wait_recv()
            so_far = (
                dd[here, band].astype(F32)
                + rc[zz, :, band].astype(F32)
                + dot_rows(spread[zz], back[zz, :, band])[:rows]
            )

            @pl.when(jnp.logical_or(is_edge, zz == outer))
            def _():
                dd[here, band] = so_far.astype(BF)

            @pl.when(jnp.logical_not(jnp.logical_or(is_edge, zz == outer)))
            def _():
                to_inner(zz, p).wait_recv()
                dd[here, band] = (so_far + edge_in[zz, :, band].astype(F32)).astype(BF)

            @pl.when(is_edge)
            def _():
                to_inner(zz, p).start()

            @pl.when(jnp.logical_not(is_edge))
            def _():
                to_owner(zz, p).start()

    def target(n):
        edge_first, inner_first = ((2, 3, 1), (0, 2, 3))
        found = jnp.where(is_edge, edge_first[n - 1], inner_first[n - 1])
        return jnp.where(2 * z < ep, found, ep - 1 - found)

    def m_x(h):
        part = pl.ds(h * wide, wide)
        return rcopy(mp.at[(1 - x) * 2 + c, :, part], mrx.at[:, part], m_s.at[2 + h], m_r.at[2 + h], xn)

    def mixer_fold():
        for xx in range(2):
            m_core(xx).wait_recv()
        mine = (1 - x) * 2 + c
        mp[mine] = (mp[mine].astype(F32) + mrc[1 - x].astype(F32)).astype(BF)

    def mixer_send(h):
        m_x(h).start()

    z_step(1)
    compacts(1)
    own_x()
    mixer()
    z_step(2)
    compacts(2)
    for name in ("eg", "eu", "ed"):
        loads[name].wait()
    compute(order[1])
    z_step(3)
    compacts(3)
    core_step(z, 2)
    shared()
    experts(z, 2)
    for side in range(2):
        d_core(z, side).start()
    compute(order[2])
    compute(order[3])
    mixer_fold()
    mixer_send(0)
    fold_z(target(1))
    mixer_send(1)
    fold_core()
    fold_z(target(2))
    fold_z(target(3))

    for h in range(HALVES):
        m_x(h).wait_recv()
    mixed = mp[t].astype(F32) + mrc[x].astype(F32) + mrx[...].astype(F32)
    scale = lax.rsqrt(jnp.mean(mixed * mixed, axis=-1, keepdims=True) + EPSILON)
    mixed_ref[...] = (mixed * scale * mgain[...]).astype(BF)

    here = lines(z, 0, c)
    d_core(z, 0).wait_recv()
    for p in range(PARTS):
        band = cols(p)
        d_x(p).wait_recv()
        total = dd[here, band].astype(F32) + rc[z, :, band].astype(F32) + rx[:, band].astype(F32)

        last_arrival(1, p).wait_recv()
        total = total + last_in[1, :, band].astype(F32)

        @pl.when(is_edge)
        def _():
            last_arrival(0, p).wait_recv()
            rows_ref[:, band] = (total + last_in[0, :, band].astype(F32)).astype(BF)

        @pl.when(jnp.logical_not(is_edge))
        def _():
            to_inner(z, p).wait_recv()
            rows_ref[:, band] = (total + edge_in[z, :, band].astype(F32)).astype(BF)

    @pl.when(has_up)
    def _():
        h_gate.wait_send()
        h_value.wait_send()

    for k in PIECES:
        c_x(k).wait_send()
    for p in range(PARTS):
        d_x(p).wait_send()
    for copy in core_pair(z, 1, c):
        copy.wait_send()
    d_core(z, 1).wait_send()

    for zz in range(ep):
        @pl.when(jnp.logical_and(has_up, zz <= z))
        def _():
            for k in PIECES:
                c_up(zz, k).wait_send()

        @pl.when(jnp.logical_and(has_down, zz >= z))
        def _():
            for k in PIECES:
                c_down(zz, k).wait_send()

        for copy in core_pair(zz, 0, c):
            copy.wait_send()
        d_core(zz, 0).wait_send()

        @pl.when(zz != z)
        def _():
            for copy in few_pair(zz):
                copy.wait_send()
            for h in range(HALVES):
                for copy in d_few(zz, h):
                    copy.wait_send()

        @pl.when(jnp.logical_and(zz != z, is_edge))
        def _():
            for p in range(PARTS):
                to_inner(zz, p).wait_send()

        @pl.when(jnp.logical_and(zz != z, jnp.logical_not(is_edge)))
        def _():
            for p in range(PARTS):
                to_owner(zz, p).wait_send()

    for xx in range(2):
        m_core(xx).wait_send()
    for h in range(HALVES):
        m_x(h).wait_send()


def fused_on_device(ep, tp, *args):
    (og, ig, iv, taps, mo, mgain, tok, egain, ids, wts, eg, eu, ed, sg, su, sd) = args
    rows, width = tok.shape
    count, columns = ig.shape
    experts = ep * tp
    cap = (3 * rows * ids.shape[1] + 2 * experts - 1) // (2 * experts)
    cap = -(-cap // 8) * 8
    slot = -(-cap // 32) * 32
    names = -(-experts // 16) * 16
    hid = eg.shape[2]
    half = sd.shape[0]
    any_spec = pl.BlockSpec(memory_space=pltpu.HBM)
    vmem = pl.BlockSpec(memory_space=pltpu.VMEM)
    dma = pltpu.SemaphoreType.DMA
    V = pltpu.VMEM
    return pl.pallas_call(
        functools.partial(fused_kernel, ep, tp, cap, slot),
        out_shape=(V((rows, width), BF), V((rows, width), BF)),
        in_specs=[any_spec] * 3 + [vmem, any_spec, vmem, any_spec, vmem, vmem, vmem] + [any_spec] * 6,
        out_specs=(vmem, vmem),
        scratch_shapes=[
            V((count, columns), BF), V((count, columns), BF), V((count, columns), BF),
            V((columns, width), BF), V((rows, width), BF),
            V((width, hid), BF), V((width, hid), BF), V((hid + half, width), BF),
            V((width, 2 * half), BF),
            V((2, 16, columns), BF), V((count + 8, columns), F32), V((count, columns), BF),
            V((experts * rows, width), BF), V((experts, names, 128), BF),
            V((tp * rows, hid + half), BF), V((experts * rows, width), BF),
            V((ep, 2 * slot, width), BF), V((ep, 2 * slot, 128), BF),
            V((ep + 1, rows, width), BF), V((ep, 2 * slot, width), BF), V((rows, width), BF),
            V((ep, rows, width), BF), V((2, rows, width), BF),
            V((tp, rows, width), BF), V((2, rows, width), BF), V((rows, width), BF),
            dma((11,)), dma((4,)),
            dma((ep, CHUNKS + 1)), dma((ep, CHUNKS + 1)), dma((ep, CHUNKS + 1)),
            dma((CHUNKS + 1,)), dma((CHUNKS + 1,)), dma((ep, 2, 2)), dma((ep, 2, 2)),
            dma((ep, 2)), dma((ep, 2)),
            dma((ep + 1,)), dma((ep + 1,)), dma((ep, HALVES, 2)), dma((ep, HALVES, 2)),
            dma((PARTS,)), dma((PARTS,)),
            dma((ep, PARTS)), dma((ep, PARTS)), dma((2, PARTS)), dma((ep, PARTS)),
            dma((2 + HALVES,)), dma((2 + HALVES,)),
        ],
        compiler_params=pltpu.CompilerParams(
            collective_id=0, has_side_effects=True, vmem_limit_bytes=60 * 1024 * 1024
        ),
    )(
        og, ig, iv, taps, mo, mgain.reshape(1, -1), tok, egain.reshape(1, -1), ids.T, wts.T, eg, eu, ed, sg, su, sd
    )


def plan(mesh):
    ep, tp = mesh.shape["ep"], mesh.shape["tp"]
    if tp == 4 and ep == 4:
        return functools.partial(fused_on_device, ep, tp)
    return on_device


def solution(mesh):
    return jax.shard_map(
        plan(mesh),
        mesh=mesh,
        in_specs=(
            P(("grp", "ep"), "tp"),
            P(("grp", "ep"), "tp"),
            P(("grp", "ep"), "tp"),
            P(),
            P("tp", None),
            P(),
            P(("grp", "ep", "tp"), None),
            P(),
            P(("grp", "ep", "tp"), None),
            P(("grp", "ep", "tp"), None),
            P(("ep", "tp"), None, None),
            P(("ep", "tp"), None, None),
            P(("ep", "tp"), None, None),
            P(None, "tp"),
            P(None, "tp"),
            P("tp", None),
        ),
        out_specs=(P(("grp", "ep", "tp"), None), P(("grp", "ep", "tp"), None)),
        check_vma=False,
    )
```

```python
import functools
import jax
import jax.numpy as jnp
from jax import lax
from jax.experimental import pallas as pl
from jax.experimental.pallas import tpu as pltpu
from jax.sharding import PartitionSpec as P

EPSILON = 1e-06


def passed_along(array, axis, by):
    size = lax.axis_size(axis)
    pairs = [(i, i + by) for i in range(size) if 0 <= i + by < size]
    return lax.ppermute(array, axis, pairs)


def rms_scale(values, gains):
    return values * lax.rsqrt(jnp.mean(values * values, axis=-1, keepdims=True) + EPSILON) * gains


def on_device(
    outer_gate,
    inner_gate,
    inner_value,
    conv_taps,
    mixer_out,
    mixer_gain,
    moe_tokens,
    expert_gain,
    route_ids,
    route_weights,
    expert_gate,
    expert_up,
    expert_down,
    shared_gate,
    shared_up,
    shared_down,
):
    columns = inner_gate.shape[1]
    kernel = lax.dynamic_slice_in_dim(conv_taps, lax.axis_index("tp") * columns, columns, 1).astype(
        jnp.float32
    )
    before_gate, before_value = passed_along((inner_gate[-2:], inner_value[-2:]), "ep", 1)
    gate_rows = jnp.concatenate([before_gate, inner_gate], axis=0).astype(jnp.float32)
    value_rows = jnp.concatenate([before_value, inner_value], axis=0).astype(jnp.float32)
    product = gate_rows * value_rows
    filtered = kernel[0] * product[:-2] + kernel[1] * product[1:-1] + kernel[2] * product[2:]
    scaled = (outer_gate.astype(jnp.float32) * filtered).astype(jnp.bfloat16)
    normed = rms_scale(moe_tokens.astype(jnp.float32), expert_gain).astype(jnp.bfloat16)
    feature_width = normed.shape[1]
    piece = lax.all_gather(normed, "tp", axis=0, tiled=True)
    gate_value = jnp.dot(piece, shared_gate, preferred_element_type=jnp.float32)
    up_value = jnp.dot(piece, shared_up, preferred_element_type=jnp.float32)
    shared_act = (jax.nn.silu(gate_value) * up_value).astype(jnp.bfloat16)
    mixer_part = jnp.dot(scaled, mixer_out, preferred_element_type=jnp.float32)
    shared_part = jnp.dot(shared_act, shared_down, preferred_element_type=jnp.float32)
    both_sums = lax.psum_scatter(
        jnp.concatenate([mixer_part, shared_part], axis=1).astype(jnp.bfloat16),
        "tp",
        scatter_dimension=0,
        tiled=True,
    ).astype(jnp.float32)
    mixed_rows = rms_scale(both_sums[:, :feature_width], mixer_gain).astype(jnp.bfloat16)
    shared_out = both_sums[:, feature_width:]
    row_count, top_count = route_ids.shape
    ep_count = lax.axis_size("ep")
    tp_count = lax.axis_size("tp")
    expert_count = ep_count * tp_count
    capacity = (3 * row_count * top_count + 2 * expert_count - 1) // (2 * expert_count)
    flat_ids = route_ids.reshape(-1)
    onehot = (flat_ids[:, None] == jnp.arange(expert_count, dtype=jnp.int32)[None, :]).astype(
        jnp.int32
    )
    slot_rank = jnp.sum(
        (jnp.cumsum(onehot, axis=0, dtype=jnp.int32) - onehot) * onehot, axis=1, dtype=jnp.int32
    )
    target = flat_ids * capacity + slot_rank
    token_of = jnp.arange(flat_ids.shape[0], dtype=jnp.int32) // top_count
    slot_token = jnp.zeros((expert_count * capacity,), jnp.int32).at[target].set(token_of)
    outgoing = normed[slot_token].reshape(expert_count, capacity, feature_width)
    arrived = lax.all_to_all(outgoing, ("ep", "tp"), split_axis=0, concat_axis=0, tiled=True)
    flat_in = arrived.reshape(expert_count * capacity, feature_width)
    gate_value = jnp.dot(flat_in, expert_gate[0], preferred_element_type=jnp.float32)
    up_value = jnp.dot(flat_in, expert_up[0], preferred_element_type=jnp.float32)
    active = (jax.nn.silu(gate_value) * up_value).astype(jnp.bfloat16)
    result = jnp.dot(active, expert_down[0], preferred_element_type=jnp.float32).astype(
        jnp.bfloat16
    )
    returned = lax.all_to_all(
        result.reshape(expert_count, capacity, feature_width),
        ("ep", "tp"),
        split_axis=0,
        concat_axis=0,
        tiled=True,
    )
    picked = returned.reshape(expert_count * capacity, feature_width)[target].astype(jnp.float32)
    weights = route_weights.reshape(-1)
    routed = jnp.sum(
        (weights[:, None] * picked).reshape(row_count, top_count, feature_width), axis=1
    )
    expert_rows = (shared_out + routed).astype(jnp.bfloat16)
    return (mixed_rows, expert_rows)


MESH = pl.DeviceIdType.MESH
BF = jnp.bfloat16
F32 = jnp.float32
CHUNKS = 2
PARTS = 4
HALVES = 2
PIECES = (CHUNKS,) + tuple(range(CHUNKS))


def dot(a, b):
    return jnp.dot(a, b, preferred_element_type=F32)


def dot_rows(a, b):
    return lax.dot_general(a, b, (((0,), (0,)), ((), ())), preferred_element_type=F32)


def fused_kernel(
    ep, tp, cap, slot,
    og_h, ig_h, iv_h, taps, mo_h, mgain, tok_h, egain, ids, wts, eg_h, eu_h, ed_h, sg_h, su_h, sd_h,
    mixed_ref, rows_ref,
    og, ig, iv, mo, tok, eg, eu, ed, sgu, halo, pbuf, scaled,
    gat, tab, act, dd, packed, spread, rc, back, rx, edge_in, last_in, mp, mrc, mrx,
    load_sem, halo_sem, gz_r, gx_r, gc_r, px_r, rc_r, q_r, rx_r, e_r, f_r, m_r, sent,
):
    z = lax.axis_index("ep")
    t = lax.axis_index("tp")
    g = lax.axis_index("grp")
    x = t // 2
    c = t % 2
    rows = tok.shape[0]
    width = tok.shape[1]
    columns = ig.shape[1]
    sub = rows // CHUNKS
    up = (g, z + 1, t)
    down = (g, z - 1, t)
    xn = (g, z, (1 - x) * 2 + c)
    pc = (g, z, x * 2 + 1 - c)
    xd = (g, z, (1 - x) * 2 + 1 - c)
    z2 = (g, (z + 2) % ep, t)
    is_edge = jnp.logical_or(z == 0, z == ep - 1)
    inner = jnp.where(2 * z < ep, z + 1, z - 1)
    outer = jnp.where(2 * z < ep, z - 1, z + 1)
    has_up = z < ep - 1
    has_down = z > 0

    loads = {}

    def load(name, src, dst):
        copy = pltpu.make_async_copy(src, dst, load_sem.at[len(loads)])
        copy.start()
        loads[name] = copy

    half = sd_h.shape[0]
    hid = eg.shape[1]
    load("tok", tok_h, tok)
    load("ig", ig_h, ig)
    load("iv", iv_h, iv)
    load("og", og_h, og)
    load("mo", mo_h, mo)
    load("sg", sg_h, sgu.at[:, pl.ds(0, half)])
    load("su", su_h, sgu.at[:, pl.ds(half, half)])
    load("sd", sd_h, ed.at[pl.ds(hid, half), :])
    load("eg", eg_h.at[0], eg)
    load("eu", eu_h.at[0], eu)
    load("ed", ed_h.at[0], ed.at[pl.ds(0, hid), :])

    barrier = pltpu.get_barrier_semaphore()
    for peer in (xn, pc, xd, z2):
        pl.semaphore_signal(barrier, inc=1, device_id=peer, device_id_type=MESH)

    @pl.when(has_up)
    def _():
        pl.semaphore_signal(barrier, inc=1, device_id=up, device_id_type=MESH)

    @pl.when(has_down)
    def _():
        pl.semaphore_signal(barrier, inc=1, device_id=down, device_id_type=MESH)

    def rcopy(src, dst, ssem, rsem, peer):
        return pltpu.make_async_remote_copy(
            src_ref=src, dst_ref=dst, send_sem=ssem, recv_sem=rsem, device_id=peer, device_id_type=MESH
        )

    def arrived(ref, sem):
        rcopy(ref, ref, sent.at[0], sem, xn).wait_recv()

    def block(zz, side, cc):
        return (zz * 2 + side) * 2 + cc

    def lines(zz, side, cc):
        return pl.ds(pl.multiple_of(block(zz, side, cc) * rows, rows), rows)

    def few(zz, cc):
        return pl.ds(pl.multiple_of(block(zz, 1, 0) * rows + cc * slot, slot), cap)

    def slots_of(cc):
        return pl.ds(pl.multiple_of(cc * slot, slot), cap)

    def piece(zz, side, cc, k):
        if k == CHUNKS:
            return tab.at[block(zz, side, cc)]
        return gat.at[pl.ds(pl.multiple_of(block(zz, side, cc) * rows + k * sub, sub), sub), :]

    def c_up(zz, k):
        return rcopy(piece(zz, 0, c, k), piece(zz, 0, c, k), sent.at[0], gz_r.at[zz, k], up)

    def c_down(zz, k):
        return rcopy(piece(zz, 0, c, k), piece(zz, 0, c, k), sent.at[0], gz_r.at[zz, k], down)

    def c_x(k):
        return rcopy(piece(z, 0, c, k), piece(z, 1, c, k), sent.at[0], gx_r.at[k], xn)

    def core_pair(zz, side, cc):
        names = tab.at[block(zz, side, cc)]
        body = gat.at[lines(zz, side, cc), :]
        at = zz if side == 0 else ep
        return (
            rcopy(body, body, sent.at[0], gc_r.at[at, 0], pc),
            rcopy(names, names, sent.at[0], gc_r.at[at, 1], pc),
        )

    def core_start(zz, side):
        for copy in core_pair(zz, side, c):
            copy.start()

    def few_pair(zz):
        return (
            rcopy(packed.at[zz, slots_of(c), :], gat.at[few(zz, c), :], sent.at[1], px_r.at[zz], xn),
            rcopy(packed.at[zz, slots_of(1 - c), :], gat.at[few(zz, c), :], sent.at[1], px_r.at[zz], xd),
        )

    for zz in range(ep):
        for e in range(2):
            back[zz, pl.ds(e * slot + cap, slot - cap), :] = jnp.zeros((slot - cap, width), BF)

    loads["tok"].wait()
    name_i = lax.broadcasted_iota(jnp.int32, (tab.shape[1], rows), 0)
    table = jnp.zeros((tab.shape[1], rows), F32)
    for k in range(ids.shape[0]):
        table = table + jnp.where(ids[k : k + 1, :] == name_i, wts[k : k + 1, :], 0.0)
    tab[block(z, 0, c)] = jnp.zeros(tab.shape[1:], BF)
    tab[block(z, 0, c), :, :rows] = table.astype(BF)
    v = tok[...].astype(F32)
    v = v * lax.rsqrt(jnp.mean(v * v, axis=-1, keepdims=True) + EPSILON) * egain[...]
    gat[lines(z, 0, c), :] = v.astype(BF)

    pl.semaphore_wait(barrier, 4 + jnp.minimum(z, 1) + jnp.minimum(ep - 1 - z, 1))

    loads["ig"].wait()
    loads["iv"].wait()
    tail = ig.shape[0] - halo.shape[1]
    edge = halo.shape[1]
    h_gate = rcopy(ig.at[pl.ds(tail, edge)], halo.at[0], sent.at[3], halo_sem.at[0], up)
    h_value = rcopy(iv.at[pl.ds(tail, edge)], halo.at[1], sent.at[3], halo_sem.at[1], up)

    @pl.when(has_up)
    def _():
        h_gate.start()
        h_value.start()

    for k in PIECES:
        @pl.when(has_up)
        def _():
            c_up(z, k).start()

        @pl.when(has_down)
        def _():
            c_down(z, k).start()

        c_x(k).start()
    core_start(z, 0)

    count = ig.shape[0]
    tile = width // PARTS

    def cols(n):
        return pl.ds(pl.multiple_of(n * tile, tile), tile)

    def m_core(xx):
        return rcopy(mp.at[xx * 2 + 1 - c], mrc.at[xx], sent.at[2], m_r.at[0], pc)

    def mixer():
        pbuf[8:, :] = ig[...].astype(F32) * iv[...].astype(F32)

        @pl.when(jnp.logical_not(has_down))
        def _():
            pbuf[:8, :] = jnp.zeros((8, columns), F32)

        @pl.when(has_down)
        def _():
            h_gate.wait_recv()
            h_value.wait_recv()
            pbuf[:8, :] = halo[0, edge - 8 :, :].astype(F32) * halo[1, edge - 8 :, :].astype(F32)

        loads["og"].wait()
        tap = taps[:, pl.ds(pl.multiple_of(t * columns, columns), columns)].astype(F32)
        filtered = (
            tap[0:1] * pbuf[6 : 6 + count, :] + tap[1:2] * pbuf[7 : 7 + count, :] + tap[2:3] * pbuf[8 : 8 + count, :]
        )
        scaled[...] = (og[...].astype(F32) * filtered).astype(BF)
        loads["mo"].wait()
        @pl.loop(0, PARTS, unroll=True)
        def _(n):
            part = dot(scaled[...], mo[:, cols(n)]).astype(BF)
            mp[:, :, cols(n)] = part.reshape(tp, rows, tile)

        for xx in range(2):
            m_core(xx).start()

    lanes = tab.shape[2]
    name_of = lax.broadcasted_iota(jnp.int32, (tab.shape[1], lanes), 0)
    before = (
        lax.broadcasted_iota(jnp.int32, (lanes, lanes), 0) < lax.broadcasted_iota(jnp.int32, (lanes, lanes), 1)
    ).astype(BF)
    slot_i = lax.broadcasted_iota(jnp.int32, (slot, lanes), 0)
    diagonal = lax.broadcasted_iota(jnp.int32, (rows, lanes), 0) == lax.broadcasted_iota(
        jnp.int32, (rows, lanes), 1
    )
    expert = z * tp + t

    def line_of(name, block_id):
        return jnp.sum(jnp.where(name_of == name, tab[block_id].astype(F32), 0.0), axis=0, keepdims=True)

    def weight_column(block_id):
        return jnp.sum(jnp.where(diagonal, line_of(expert, block_id), 0.0), axis=1, keepdims=True)

    def compact(zz):
        marks = []
        for e in range(2):
            weight = line_of(z * tp + (1 - x) * 2 + e, block(zz, 0, c))
            named = weight > 0
            ahead = dot(jnp.broadcast_to(named, (8, lanes)).astype(F32).astype(BF), before)[0:1]
            hit = jnp.logical_and(slot_i == ahead.astype(jnp.int32), named)
            marks.append(hit.astype(F32))
            spread[zz, pl.ds(e * slot, slot), :] = jnp.where(hit, weight, 0.0).astype(BF)
        mark = jnp.concatenate(marks, axis=0).astype(BF)[:, :rows]

        @pl.loop(0, PARTS, unroll=True)
        def _(n):
            packed[zz, :, cols(n)] = dot(mark, gat[lines(zz, 0, c), cols(n)]).astype(BF)

        for copy in few_pair(zz):
            copy.start()

    def z_step(s):
        for k in PIECES:
            @pl.when(z >= s)
            def _():
                c_up(z - s, k).wait_recv()

                @pl.when(has_up)
                def _():
                    c_up(z - s, k).start()

            @pl.when(z + s < ep)
            def _():
                c_down(z + s, k).wait_recv()

                @pl.when(has_down)
                def _():
                    c_down(z + s, k).start()

        @pl.when(z >= s)
        def _():
            core_start(z - s, 0)

        @pl.when(z + s < ep)
        def _():
            core_start(z + s, 0)

    def compacts(s):
        @pl.when(z >= s)
        def _():
            compact(z - s)

        @pl.when(z + s < ep)
        def _():
            compact(z + s)

    def own_x():
        for k in PIECES:
            c_x(k).wait_recv()
        core_start(z, 1)

    def core_step(zz, sides):
        for side in range(sides):
            for copy in core_pair(zz, side, 1 - c):
                copy.wait_recv()
        if sides == 1:
            arrived(gat.at[pl.ds(pl.multiple_of(block(zz, 1, 0) * rows, rows), 2 * cap), :], px_r.at[zz])

    def nth(n):
        near = jnp.minimum(z, ep - 1 - z)
        d = (n + 1) // 2
        side = z - d if n % 2 else z + d
        far = jnp.where(z < ep - 1 - z, n, ep - 1 - n)
        return jnp.where(n <= 2 * near, side, far)

    order = [nth(n) for n in range(ep)]

    def shared():
        for name in ("sg", "su", "sd"):
            loads[name].wait()
        own = pl.ds(pl.multiple_of(block(z, 0, 0) * rows, tp * rows), tp * rows)
        hidden = dot(gat[own, :], sgu[...])
        gate, value = hidden[:, :half], hidden[:, half:]
        act[:, hid:] = (gate / (1.0 + jnp.exp(-gate)) * value).astype(BF)

    def experts(zz, sides):
        depth = hid + half if sides == 2 else hid
        weights = [weight_column(block(zz, side, cc)) for side in range(sides) for cc in range(2)]
        if sides == 1:
            weights.append(jnp.ones((2 * slot, 1), F32))
        weight = jnp.concatenate(weights, axis=0)
        amount = weight.shape[0]
        span = pl.ds(pl.multiple_of(block(zz, 0, 0) * rows, tp * rows), amount)
        step = 256 if hid % 256 == 0 else hid

        @pl.loop(0, hid // step, unroll=True)
        def _(n):
            col = pl.ds(pl.multiple_of(n * step, step), step)
            gate = dot(gat[span, :], eg[:, col])
            value = dot(gat[span, :], eu[:, col])
            act[:amount, col] = (gate / (1.0 + jnp.exp(-gate)) * value * weight).astype(BF)

        @pl.loop(0, PARTS, unroll=True)
        def _(n):
            dd[span, cols(n)] = dot(act[:amount, :depth], ed[:depth, cols(n)]).astype(BF)

    def d_core(zz, side):
        at = zz if side == 0 else ep
        return rcopy(dd.at[lines(zz, side, 1 - c), :], rc.at[at], sent.at[1], rc_r.at[at], pc)

    wide = width // HALVES

    def d_few(zz, h):
        part = pl.ds(h * wide, wide)
        return (
            rcopy(
                dd.at[few(zz, c), part], back.at[zz, slots_of(c), part],
                sent.at[1], q_r.at[zz, h], xn,
            ),
            rcopy(
                dd.at[few(zz, 1 - c), part], back.at[zz, slots_of(c), part],
                sent.at[1], q_r.at[zz, h], xd,
            ),
        )

    def d_x(p):
        return rcopy(dd.at[lines(z, 1, c), cols(p)], rx.at[:, cols(p)], sent.at[2], rx_r.at[p], xn)

    def to_inner(zz, p):
        src = dd.at[lines(zz, 0, c), cols(p)]
        return rcopy(src, edge_in.at[zz, :, cols(p)], sent.at[2], e_r.at[zz, p], (g, inner, t))

    def to_owner(zz, p):
        owner_is_edge = jnp.logical_or(zz == 0, zz == ep - 1)
        place = jnp.where(jnp.logical_and(owner_is_edge, zz == outer), 0, 1)
        src = dd.at[lines(zz, 0, c), cols(p)]
        return rcopy(src, last_in.at[place, :, cols(p)], sent.at[2], f_r.at[place, p], (g, zz, t))

    def last_arrival(place, p):
        here = last_in.at[place, :, cols(p)]
        return rcopy(here, here, sent.at[2], f_r.at[place, p], xn)

    def compute(zz):
        core_step(zz, 1)
        experts(zz, 1)
        d_core(zz, 0).start()

    def few_send(zz):
        for h in range(HALVES):
            for copy in d_few(zz, h):
                copy.start()

    def fold_core():
        d_core(z, 1).wait_recv()
        there = lines(z, 1, c)
        dd[there, :] = (dd[there, :].astype(F32) + rc[ep].astype(F32)).astype(BF)
        for p in range(PARTS):
            d_x(p).start()

    def fold_z(zz):
        here = lines(zz, 0, c)
        d_core(zz, 0).wait_recv()
        for p in range(PARTS):
            band = cols(p)
            if p % (PARTS // HALVES) == 0:
                h = p // (PARTS // HALVES)
                arrived(back.at[zz, pl.ds(0, 2 * cap), pl.ds(h * wide, wide)], q_r.at[zz, h])
            so_far = (
                dd[here, band].astype(F32)
                + rc[zz, :, band].astype(F32)
                + dot_rows(spread[zz], back[zz, :, band])[:rows]
            )

            @pl.when(jnp.logical_or(is_edge, zz == outer))
            def _():
                dd[here, band] = so_far.astype(BF)

            @pl.when(jnp.logical_not(jnp.logical_or(is_edge, zz == outer)))
            def _():
                to_inner(zz, p).wait_recv()
                dd[here, band] = (so_far + edge_in[zz, :, band].astype(F32)).astype(BF)

            @pl.when(is_edge)
            def _():
                to_inner(zz, p).start()

            @pl.when(jnp.logical_not(is_edge))
            def _():
                to_owner(zz, p).start()

    def target(n):
        edge_first, inner_first = ((2, 3, 1), (0, 2, 3))
        found = jnp.where(is_edge, edge_first[n - 1], inner_first[n - 1])
        return jnp.where(2 * z < ep, found, ep - 1 - found)

    def m_x(h):
        part = pl.ds(h * wide, wide)
        return rcopy(mp.at[(1 - x) * 2 + c, :, part], mrx.at[:, part], sent.at[2], m_r.at[1 + h], xn)

    def mixer_fold():
        arrived(mrc, m_r.at[0])
        mine = (1 - x) * 2 + c
        mp[mine] = (mp[mine].astype(F32) + mrc[1 - x].astype(F32)).astype(BF)

    def mixer_send(h):
        m_x(h).start()

    z_step(1)
    own_x()
    compacts(1)
    z_step(2)
    compacts(2)
    mixer()
    for name in ("eg", "eu", "ed"):
        loads[name].wait()
    compute(order[1])
    few_send(order[1])
    z_step(3)
    compacts(3)
    compute(order[2])
    core_step(z, 2)
    shared()
    experts(z, 2)
    for side in range(2):
        d_core(z, side).start()
    few_send(order[2])
    compute(order[3])
    few_send(order[3])
    mixer_fold()
    mixer_send(0)
    mixer_send(1)
    fold_core()
    fold_z(target(1))
    fold_z(target(2))
    fold_z(target(3))
    for h in range(HALVES):
        m_x(h).wait_recv()
    mixed = mp[t].astype(F32) + mrc[x].astype(F32) + mrx[...].astype(F32)
    scale = lax.rsqrt(jnp.mean(mixed * mixed, axis=-1, keepdims=True) + EPSILON)
    mixed_ref[...] = (mixed * scale * mgain[...]).astype(BF)

    here = lines(z, 0, c)
    d_core(z, 0).wait_recv()
    for p in range(PARTS):
        band = cols(p)
        d_x(p).wait_recv()
        total = dd[here, band].astype(F32) + rc[z, :, band].astype(F32) + rx[:, band].astype(F32)

        last_arrival(1, p).wait_recv()
        total = total + last_in[1, :, band].astype(F32)

        @pl.when(is_edge)
        def _():
            last_arrival(0, p).wait_recv()
            rows_ref[:, band] = (total + last_in[0, :, band].astype(F32)).astype(BF)

        @pl.when(jnp.logical_not(is_edge))
        def _():
            to_inner(z, p).wait_recv()
            rows_ref[:, band] = (total + edge_in[z, :, band].astype(F32)).astype(BF)

    def left(ref, sem):
        rcopy(ref, ref, sem, m_r.at[0], xn).wait_send()

    def drain():
        @pl.when(has_up)
        def _():
            left(halo, sent.at[3])

        for edge_chip, moved in ((True, 1), (False, 2 * ep - 3)):
            total_blocks = moved + ep + 2

            @pl.when(is_edge == edge_chip)
            def _():
                left(gat.at[pl.ds(0, total_blocks * rows), :], sent.at[0])
                left(tab.at[pl.ds(0, total_blocks)], sent.at[0])

        slots = 2 * (ep - 1) * 2 * cap
        left(gat.at[pl.ds(0, slots + (ep + 1) * rows), :], sent.at[1])
        left(gat.at[pl.ds(0, (1 + ep - 1 + 3) * rows), :], sent.at[2])

    drain()


def store_rows(mixed_ref, rows_ref, mixed_out, rows_out, sem):
    copies = [
        pltpu.make_async_copy(mixed_ref, mixed_out, sem.at[0]),
        pltpu.make_async_copy(rows_ref, rows_out, sem.at[1]),
    ]
    for copy in copies:
        copy.start()
    for copy in copies:
        copy.wait()


def fused_on_device(ep, tp, *args):
    (og, ig, iv, taps, mo, mgain, tok, egain, ids, wts, eg, eu, ed, sg, su, sd) = args
    rows, width = tok.shape
    count, columns = ig.shape
    experts = ep * tp
    cap = (3 * rows * ids.shape[1] + 2 * experts - 1) // (2 * experts)
    cap = -(-cap // 8) * 8
    slot = -(-cap // 32) * 32
    names = -(-experts // 16) * 16
    hid = eg.shape[2]
    half = sd.shape[0]
    any_spec = pl.BlockSpec(memory_space=pltpu.HBM)
    vmem = pl.BlockSpec(memory_space=pltpu.VMEM)
    dma = pltpu.SemaphoreType.DMA
    V = pltpu.VMEM
    mixed, summed = pl.pallas_call(
        functools.partial(fused_kernel, ep, tp, cap, slot),
        out_shape=(V((rows, width), BF), V((rows, width), BF)),
        in_specs=[any_spec] * 3 + [vmem, any_spec, vmem, any_spec, vmem, vmem, vmem] + [any_spec] * 6,
        out_specs=(vmem, vmem),
        scratch_shapes=[
            V((count, columns), BF), V((count, columns), BF), V((count, columns), BF),
            V((columns, width), BF), V((rows, width), BF),
            V((width, hid), BF), V((width, hid), BF), V((hid + half, width), BF),
            V((width, 2 * half), BF),
            V((2, 16, columns), BF), V((count + 8, columns), F32), V((count, columns), BF),
            V((experts * rows, width), BF), V((experts, names, 128), BF),
            V((tp * rows, hid + half), BF), V((experts * rows, width), BF),
            V((ep, 2 * slot, width), BF), V((ep, 2 * slot, 128), BF),
            V((ep + 1, rows, width), BF), V((ep, 2 * slot, width), BF), V((rows, width), BF),
            V((ep, rows, width), BF), V((2, rows, width), BF),
            V((tp, rows, width), BF), V((2, rows, width), BF), V((rows, width), BF),
            dma((11,)), dma((2,)), dma((ep, CHUNKS + 1)), dma((CHUNKS + 1,)), dma((ep + 1, 2)), dma((ep,)),
            dma((ep + 1,)), dma((ep, HALVES)), dma((PARTS,)), dma((ep, PARTS)), dma((2, PARTS)),
            dma((1 + HALVES,)), dma((4,)),
        ],
        compiler_params=pltpu.CompilerParams(
            collective_id=0, has_side_effects=True, vmem_limit_bytes=60 * 1024 * 1024
        ),
    )(
        og, ig, iv, taps, mo, mgain.reshape(1, -1), tok, egain.reshape(1, -1), ids.T, wts.T, eg, eu, ed, sg, su, sd
    )
    out = jax.ShapeDtypeStruct((rows, width), BF)
    return pl.pallas_call(
        store_rows,
        out_shape=(out, out),
        in_specs=[vmem, vmem],
        out_specs=(any_spec, any_spec),
        scratch_shapes=[dma((2,))],
    )(
        pltpu.with_memory_space_constraint(mixed, pltpu.VMEM),
        pltpu.with_memory_space_constraint(summed, pltpu.VMEM),
    )


def plan(mesh):
    ep, tp = mesh.shape["ep"], mesh.shape["tp"]
    if tp == 4 and ep == 4:
        return functools.partial(fused_on_device, ep, tp)
    return on_device


def solution(mesh):
    return jax.shard_map(
        plan(mesh),
        mesh=mesh,
        in_specs=(
            P(("grp", "ep"), "tp"),
            P(("grp", "ep"), "tp"),
            P(("grp", "ep"), "tp"),
            P(),
            P("tp", None),
            P(),
            P(("grp", "ep", "tp"), None),
            P(),
            P(("grp", "ep", "tp"), None),
            P(("grp", "ep", "tp"), None),
            P(("ep", "tp"), None, None),
            P(("ep", "tp"), None, None),
            P(("ep", "tp"), None, None),
            P(None, "tp"),
            P(None, "tp"),
            P("tp", None),
        ),
        out_specs=(P(("grp", "ep", "tp"), None), P(("grp", "ep", "tp"), None)),
        check_vma=False,
    )
```

```python
import functools
import jax
import jax.numpy as jnp
from jax import lax
from jax.experimental import pallas as pl
from jax.experimental.pallas import tpu as pltpu
from jax.sharding import PartitionSpec as P

EPSILON = 1e-06


def passed_along(array, axis, by):
    size = lax.axis_size(axis)
    pairs = [(i, i + by) for i in range(size) if 0 <= i + by < size]
    return lax.ppermute(array, axis, pairs)


def rms_scale(values, gains):
    return values * lax.rsqrt(jnp.mean(values * values, axis=-1, keepdims=True) + EPSILON) * gains


def on_device(
    outer_gate,
    inner_gate,
    inner_value,
    conv_taps,
    mixer_out,
    mixer_gain,
    moe_tokens,
    expert_gain,
    route_ids,
    route_weights,
    expert_gate,
    expert_up,
    expert_down,
    shared_gate,
    shared_up,
    shared_down,
):
    columns = inner_gate.shape[1]
    kernel = lax.dynamic_slice_in_dim(conv_taps, lax.axis_index("tp") * columns, columns, 1).astype(
        jnp.float32
    )
    before_gate, before_value = passed_along((inner_gate[-2:], inner_value[-2:]), "ep", 1)
    gate_rows = jnp.concatenate([before_gate, inner_gate], axis=0).astype(jnp.float32)
    value_rows = jnp.concatenate([before_value, inner_value], axis=0).astype(jnp.float32)
    product = gate_rows * value_rows
    filtered = kernel[0] * product[:-2] + kernel[1] * product[1:-1] + kernel[2] * product[2:]
    scaled = (outer_gate.astype(jnp.float32) * filtered).astype(jnp.bfloat16)
    normed = rms_scale(moe_tokens.astype(jnp.float32), expert_gain).astype(jnp.bfloat16)
    feature_width = normed.shape[1]
    piece = lax.all_gather(normed, "tp", axis=0, tiled=True)
    gate_value = jnp.dot(piece, shared_gate, preferred_element_type=jnp.float32)
    up_value = jnp.dot(piece, shared_up, preferred_element_type=jnp.float32)
    shared_act = (jax.nn.silu(gate_value) * up_value).astype(jnp.bfloat16)
    mixer_part = jnp.dot(scaled, mixer_out, preferred_element_type=jnp.float32)
    shared_part = jnp.dot(shared_act, shared_down, preferred_element_type=jnp.float32)
    both_sums = lax.psum_scatter(
        jnp.concatenate([mixer_part, shared_part], axis=1).astype(jnp.bfloat16),
        "tp",
        scatter_dimension=0,
        tiled=True,
    ).astype(jnp.float32)
    mixed_rows = rms_scale(both_sums[:, :feature_width], mixer_gain).astype(jnp.bfloat16)
    shared_out = both_sums[:, feature_width:]
    row_count, top_count = route_ids.shape
    ep_count = lax.axis_size("ep")
    tp_count = lax.axis_size("tp")
    expert_count = ep_count * tp_count
    capacity = (3 * row_count * top_count + 2 * expert_count - 1) // (2 * expert_count)
    flat_ids = route_ids.reshape(-1)
    onehot = (flat_ids[:, None] == jnp.arange(expert_count, dtype=jnp.int32)[None, :]).astype(
        jnp.int32
    )
    slot_rank = jnp.sum(
        (jnp.cumsum(onehot, axis=0, dtype=jnp.int32) - onehot) * onehot, axis=1, dtype=jnp.int32
    )
    target = flat_ids * capacity + slot_rank
    token_of = jnp.arange(flat_ids.shape[0], dtype=jnp.int32) // top_count
    slot_token = jnp.zeros((expert_count * capacity,), jnp.int32).at[target].set(token_of)
    outgoing = normed[slot_token].reshape(expert_count, capacity, feature_width)
    arrived = lax.all_to_all(outgoing, ("ep", "tp"), split_axis=0, concat_axis=0, tiled=True)
    flat_in = arrived.reshape(expert_count * capacity, feature_width)
    gate_value = jnp.dot(flat_in, expert_gate[0], preferred_element_type=jnp.float32)
    up_value = jnp.dot(flat_in, expert_up[0], preferred_element_type=jnp.float32)
    active = (jax.nn.silu(gate_value) * up_value).astype(jnp.bfloat16)
    result = jnp.dot(active, expert_down[0], preferred_element_type=jnp.float32).astype(
        jnp.bfloat16
    )
    returned = lax.all_to_all(
        result.reshape(expert_count, capacity, feature_width),
        ("ep", "tp"),
        split_axis=0,
        concat_axis=0,
        tiled=True,
    )
    picked = returned.reshape(expert_count * capacity, feature_width)[target].astype(jnp.float32)
    weights = route_weights.reshape(-1)
    routed = jnp.sum(
        (weights[:, None] * picked).reshape(row_count, top_count, feature_width), axis=1
    )
    expert_rows = (shared_out + routed).astype(jnp.bfloat16)
    return (mixed_rows, expert_rows)


MESH = pl.DeviceIdType.MESH
BF = jnp.bfloat16
F32 = jnp.float32
CHUNKS = 2
PARTS = 4
HALVES = 2
PIECES = (CHUNKS,) + tuple(range(CHUNKS))


def dot(a, b):
    return jnp.dot(a, b, preferred_element_type=F32)


def dot_rows(a, b):
    return lax.dot_general(a, b, (((0,), (0,)), ((), ())), preferred_element_type=F32)


def fused_kernel(
    ep, tp, cap, slot,
    og_h, ig_h, iv_h, taps_h, mo_h, mgain_h, tok_h, egain_h, ids_h, wts_h, eg_h, eu_h, ed_h, sg_h, su_h, sd_h,
    mixed_ref, rows_ref,
    og, ig, iv, mo, tok, taps, mgain, egain, ids, wts, eg, eu, ed, sgu, halo, pbuf, scaled,
    gat, tab, act, dd, packed, spread, rc, back, rx, edge_in, last_in, mp, mrc, mrx,
    load_sem, halo_sem, gz_r, gx_r, gc_r, px_r, rc_r, q_r, rx_r, e_r, f_r, m_r, sent,
):
    z = lax.axis_index("ep")
    t = lax.axis_index("tp")
    g = lax.axis_index("grp")
    x = t // 2
    c = t % 2
    rows = tok.shape[0]
    width = tok.shape[1]
    columns = ig.shape[1]
    sub = rows // CHUNKS
    up = (g, z + 1, t)
    down = (g, z - 1, t)
    xn = (g, z, (1 - x) * 2 + c)
    pc = (g, z, x * 2 + 1 - c)
    xd = (g, z, (1 - x) * 2 + 1 - c)
    z2 = (g, (z + 2) % ep, t)
    is_edge = jnp.logical_or(z == 0, z == ep - 1)
    inner = jnp.where(2 * z < ep, z + 1, z - 1)
    outer = jnp.where(2 * z < ep, z - 1, z + 1)
    has_up = z < ep - 1
    has_down = z > 0

    loads = {}

    def load(name, src, dst):
        copy = pltpu.make_async_copy(src, dst, load_sem.at[len(loads)])
        copy.start()
        loads[name] = copy

    half = sd_h.shape[0]
    hid = eg.shape[1]
    load("tok", tok_h, tok)
    load("egain", egain_h, egain)
    load("ids", ids_h, ids)
    load("wts", wts_h, wts)
    load("ig", ig_h, ig)
    load("iv", iv_h, iv)
    load("taps", taps_h, taps)
    load("og", og_h, og)
    load("mo", mo_h, mo)
    load("sg", sg_h, sgu.at[:, pl.ds(0, half)])
    load("su", su_h, sgu.at[:, pl.ds(half, half)])
    load("sd", sd_h, ed.at[pl.ds(hid, half), :])
    load("eg", eg_h.at[0], eg)
    load("eu", eu_h.at[0], eu)
    load("ed", ed_h.at[0], ed.at[pl.ds(0, hid), :])
    load("mgain", mgain_h, mgain)

    barrier = pltpu.get_barrier_semaphore()
    for peer in (xn, pc, xd, z2):
        pl.semaphore_signal(barrier, inc=1, device_id=peer, device_id_type=MESH)

    @pl.when(has_up)
    def _():
        pl.semaphore_signal(barrier, inc=1, device_id=up, device_id_type=MESH)

    @pl.when(has_down)
    def _():
        pl.semaphore_signal(barrier, inc=1, device_id=down, device_id_type=MESH)

    def rcopy(src, dst, ssem, rsem, peer):
        return pltpu.make_async_remote_copy(
            src_ref=src, dst_ref=dst, send_sem=ssem, recv_sem=rsem, device_id=peer, device_id_type=MESH
        )

    def arrived(ref, sem):
        rcopy(ref, ref, sent.at[0], sem, xn).wait_recv()

    def block(zz, side, cc):
        return (zz * 2 + side) * 2 + cc

    def lines(zz, side, cc):
        return pl.ds(pl.multiple_of(block(zz, side, cc) * rows, rows), rows)

    def few(zz, cc):
        return pl.ds(pl.multiple_of(block(zz, 1, 0) * rows + cc * slot, slot), cap)

    def slots_of(cc):
        return pl.ds(pl.multiple_of(cc * slot, slot), cap)

    def piece(zz, side, cc, k):
        if k == CHUNKS:
            return tab.at[block(zz, side, cc)]
        return gat.at[pl.ds(pl.multiple_of(block(zz, side, cc) * rows + k * sub, sub), sub), :]

    def c_up(zz, k):
        return rcopy(piece(zz, 0, c, k), piece(zz, 0, c, k), sent.at[0], gz_r.at[zz, k], up)

    def c_down(zz, k):
        return rcopy(piece(zz, 0, c, k), piece(zz, 0, c, k), sent.at[0], gz_r.at[zz, k], down)

    def c_x(k):
        return rcopy(piece(z, 0, c, k), piece(z, 1, c, k), sent.at[0], gx_r.at[k], xn)

    def core_pair(zz, side, cc):
        names = tab.at[block(zz, side, cc)]
        body = gat.at[lines(zz, side, cc), :]
        at = zz if side == 0 else ep
        return (
            rcopy(body, body, sent.at[0], gc_r.at[at, 0], pc),
            rcopy(names, names, sent.at[0], gc_r.at[at, 1], pc),
        )

    def core_start(zz, side):
        for copy in core_pair(zz, side, c):
            copy.start()

    def few_pair(zz):
        return (
            rcopy(packed.at[zz, slots_of(c), :], gat.at[few(zz, c), :], sent.at[1], px_r.at[zz], xn),
            rcopy(packed.at[zz, slots_of(1 - c), :], gat.at[few(zz, c), :], sent.at[1], px_r.at[zz], xd),
        )

    for zz in range(ep):
        for e in range(2):
            back[zz, pl.ds(e * slot + cap, slot - cap), :] = jnp.zeros((slot - cap, width), BF)

    for name in ("tok", "egain", "ids", "wts"):
        loads[name].wait()
    name_i = lax.broadcasted_iota(jnp.int32, (tab.shape[1], rows), 0)
    table = jnp.zeros((tab.shape[1], rows), F32)
    for k in range(ids.shape[0]):
        table = table + jnp.where(ids[k : k + 1, :] == name_i, wts[k : k + 1, :], 0.0)
    tab[block(z, 0, c)] = jnp.zeros(tab.shape[1:], BF)
    tab[block(z, 0, c), :, :rows] = table.astype(BF)
    v = tok[...].astype(F32)
    v = v * lax.rsqrt(jnp.mean(v * v, axis=-1, keepdims=True) + EPSILON) * egain[...]
    gat[lines(z, 0, c), :] = v.astype(BF)

    pl.semaphore_wait(barrier, 4 + jnp.minimum(z, 1) + jnp.minimum(ep - 1 - z, 1))

    loads["ig"].wait()
    loads["iv"].wait()
    tail = ig.shape[0] - halo.shape[1]
    edge = halo.shape[1]
    h_gate = rcopy(ig.at[pl.ds(tail, edge)], halo.at[0], sent.at[3], halo_sem.at[0], up)
    h_value = rcopy(iv.at[pl.ds(tail, edge)], halo.at[1], sent.at[3], halo_sem.at[1], up)

    @pl.when(has_up)
    def _():
        h_gate.start()
        h_value.start()

    for k in PIECES:
        @pl.when(has_up)
        def _():
            c_up(z, k).start()

        @pl.when(has_down)
        def _():
            c_down(z, k).start()

        c_x(k).start()
    core_start(z, 0)

    count = ig.shape[0]
    tile = width // PARTS

    def cols(n):
        return pl.ds(pl.multiple_of(n * tile, tile), tile)

    def m_core(xx):
        return rcopy(mp.at[xx * 2 + 1 - c], mrc.at[xx], sent.at[2], m_r.at[0], pc)

    def mixer():
        pbuf[8:, :] = ig[...].astype(F32) * iv[...].astype(F32)

        @pl.when(jnp.logical_not(has_down))
        def _():
            pbuf[:8, :] = jnp.zeros((8, columns), F32)

        @pl.when(has_down)
        def _():
            h_gate.wait_recv()
            h_value.wait_recv()
            pbuf[:8, :] = halo[0, edge - 8 :, :].astype(F32) * halo[1, edge - 8 :, :].astype(F32)

        loads["og"].wait()
        loads["taps"].wait()
        tap = taps[:, pl.ds(pl.multiple_of(t * columns, columns), columns)].astype(F32)
        filtered = (
            tap[0:1] * pbuf[6 : 6 + count, :] + tap[1:2] * pbuf[7 : 7 + count, :] + tap[2:3] * pbuf[8 : 8 + count, :]
        )
        scaled[...] = (og[...].astype(F32) * filtered).astype(BF)
        loads["mo"].wait()
        @pl.loop(0, PARTS, unroll=True)
        def _(n):
            part = dot(scaled[...], mo[:, cols(n)]).astype(BF)
            mp[:, :, cols(n)] = part.reshape(tp, rows, tile)

        for xx in range(2):
            m_core(xx).start()

    lanes = tab.shape[2]
    name_of = lax.broadcasted_iota(jnp.int32, (tab.shape[1], lanes), 0)
    before = (
        lax.broadcasted_iota(jnp.int32, (lanes, lanes), 0) < lax.broadcasted_iota(jnp.int32, (lanes, lanes), 1)
    ).astype(BF)
    slot_i = lax.broadcasted_iota(jnp.int32, (slot, lanes), 0)
    diagonal = lax.broadcasted_iota(jnp.int32, (rows, lanes), 0) == lax.broadcasted_iota(
        jnp.int32, (rows, lanes), 1
    )
    expert = z * tp + t

    def line_of(name, block_id):
        return jnp.sum(jnp.where(name_of == name, tab[block_id].astype(F32), 0.0), axis=0, keepdims=True)

    def weight_column(block_id):
        return jnp.sum(jnp.where(diagonal, line_of(expert, block_id), 0.0), axis=1, keepdims=True)

    def compact(zz):
        marks = []
        for e in range(2):
            weight = line_of(z * tp + (1 - x) * 2 + e, block(zz, 0, c))
            named = weight > 0
            ahead = dot(jnp.broadcast_to(named, (8, lanes)).astype(F32).astype(BF), before)[0:1]
            hit = jnp.logical_and(slot_i == ahead.astype(jnp.int32), named)
            marks.append(hit.astype(F32))
            spread[zz, pl.ds(e * slot, slot), :] = jnp.where(hit, weight, 0.0).astype(BF)
        mark = jnp.concatenate(marks, axis=0).astype(BF)[:, :rows]

        @pl.loop(0, PARTS, unroll=True)
        def _(n):
            packed[zz, :, cols(n)] = dot(mark, gat[lines(zz, 0, c), cols(n)]).astype(BF)

        for copy in few_pair(zz):
            copy.start()

    def z_step(s):
        for k in PIECES:
            @pl.when(z >= s)
            def _():
                c_up(z - s, k).wait_recv()

                @pl.when(has_up)
                def _():
                    c_up(z - s, k).start()

            @pl.when(z + s < ep)
            def _():
                c_down(z + s, k).wait_recv()

                @pl.when(has_down)
                def _():
                    c_down(z + s, k).start()

        @pl.when(z >= s)
        def _():
            core_start(z - s, 0)

        @pl.when(z + s < ep)
        def _():
            core_start(z + s, 0)

    def compacts(s):
        @pl.when(z >= s)
        def _():
            compact(z - s)

        @pl.when(z + s < ep)
        def _():
            compact(z + s)

    def own_x():
        for k in PIECES:
            c_x(k).wait_recv()
        core_start(z, 1)

    def core_step(zz, sides):
        for side in range(sides):
            for copy in core_pair(zz, side, 1 - c):
                copy.wait_recv()
        if sides == 1:
            arrived(gat.at[pl.ds(pl.multiple_of(block(zz, 1, 0) * rows, rows), 2 * cap), :], px_r.at[zz])

    def nth(n):
        near = jnp.minimum(z, ep - 1 - z)
        d = (n + 1) // 2
        side = z - d if n % 2 else z + d
        far = jnp.where(z < ep - 1 - z, n, ep - 1 - n)
        return jnp.where(n <= 2 * near, side, far)

    order = [nth(n) for n in range(ep)]

    def shared():
        for name in ("sg", "su", "sd"):
            loads[name].wait()
        own = pl.ds(pl.multiple_of(block(z, 0, 0) * rows, tp * rows), tp * rows)
        hidden = dot(gat[own, :], sgu[...])
        gate, value = hidden[:, :half], hidden[:, half:]
        act[:, hid:] = (gate / (1.0 + jnp.exp(-gate)) * value).astype(BF)

    def experts(zz, sides):
        depth = hid + half if sides == 2 else hid
        weights = [weight_column(block(zz, side, cc)) for side in range(sides) for cc in range(2)]
        if sides == 1:
            weights.append(jnp.ones((2 * slot, 1), F32))
        weight = jnp.concatenate(weights, axis=0)
        amount = weight.shape[0]
        span = pl.ds(pl.multiple_of(block(zz, 0, 0) * rows, tp * rows), amount)
        step = 256 if hid % 256 == 0 else hid

        @pl.loop(0, hid // step, unroll=True)
        def _(n):
            col = pl.ds(pl.multiple_of(n * step, step), step)
            gate = dot(gat[span, :], eg[:, col])
            value = dot(gat[span, :], eu[:, col])
            act[:amount, col] = (gate / (1.0 + jnp.exp(-gate)) * value * weight).astype(BF)

        @pl.loop(0, PARTS, unroll=True)
        def _(n):
            dd[span, cols(n)] = dot(act[:amount, :depth], ed[:depth, cols(n)]).astype(BF)

    def d_core(zz, side):
        at = zz if side == 0 else ep
        return rcopy(dd.at[lines(zz, side, 1 - c), :], rc.at[at], sent.at[1], rc_r.at[at], pc)

    wide = width // HALVES

    def d_few(zz, h):
        part = pl.ds(h * wide, wide)
        return (
            rcopy(
                dd.at[few(zz, c), part], back.at[zz, slots_of(c), part],
                sent.at[1], q_r.at[zz, h], xn,
            ),
            rcopy(
                dd.at[few(zz, 1 - c), part], back.at[zz, slots_of(c), part],
                sent.at[1], q_r.at[zz, h], xd,
            ),
        )

    def d_x(p):
        return rcopy(dd.at[lines(z, 1, c), cols(p)], rx.at[:, cols(p)], sent.at[2], rx_r.at[p], xn)

    def to_inner(zz, p):
        src = dd.at[lines(zz, 0, c), cols(p)]
        return rcopy(src, edge_in.at[zz, :, cols(p)], sent.at[2], e_r.at[zz, p], (g, inner, t))

    def to_owner(zz, p):
        owner_is_edge = jnp.logical_or(zz == 0, zz == ep - 1)
        place = jnp.where(jnp.logical_and(owner_is_edge, zz == outer), 0, 1)
        src = dd.at[lines(zz, 0, c), cols(p)]
        return rcopy(src, last_in.at[place, :, cols(p)], sent.at[2], f_r.at[place, p], (g, zz, t))

    def last_arrival(place, p):
        here = last_in.at[place, :, cols(p)]
        return rcopy(here, here, sent.at[2], f_r.at[place, p], xn)

    def compute(zz):
        core_step(zz, 1)
        experts(zz, 1)
        d_core(zz, 0).start()

    def few_send(zz):
        for h in range(HALVES):
            for copy in d_few(zz, h):
                copy.start()

    def fold_core():
        d_core(z, 1).wait_recv()
        there = lines(z, 1, c)
        dd[there, :] = (dd[there, :].astype(F32) + rc[ep].astype(F32)).astype(BF)
        for p in range(PARTS):
            d_x(p).start()

    def fold_z(zz):
        here = lines(zz, 0, c)
        d_core(zz, 0).wait_recv()
        for p in range(PARTS):
            band = cols(p)
            if p % (PARTS // HALVES) == 0:
                h = p // (PARTS // HALVES)
                arrived(back.at[zz, pl.ds(0, 2 * cap), pl.ds(h * wide, wide)], q_r.at[zz, h])
            so_far = (
                dd[here, band].astype(F32)
                + rc[zz, :, band].astype(F32)
                + dot_rows(spread[zz], back[zz, :, band])[:rows]
            )

            @pl.when(jnp.logical_or(is_edge, zz == outer))
            def _():
                dd[here, band] = so_far.astype(BF)

            @pl.when(jnp.logical_not(jnp.logical_or(is_edge, zz == outer)))
            def _():
                to_inner(zz, p).wait_recv()
                dd[here, band] = (so_far + edge_in[zz, :, band].astype(F32)).astype(BF)

            @pl.when(is_edge)
            def _():
                to_inner(zz, p).start()

            @pl.when(jnp.logical_not(is_edge))
            def _():
                to_owner(zz, p).start()

    def target(n):
        edge_first, inner_first = ((2, 3, 1), (0, 2, 3))
        found = jnp.where(is_edge, edge_first[n - 1], inner_first[n - 1])
        return jnp.where(2 * z < ep, found, ep - 1 - found)

    def m_x(h):
        part = pl.ds(h * wide, wide)
        return rcopy(mp.at[(1 - x) * 2 + c, :, part], mrx.at[:, part], sent.at[2], m_r.at[1 + h], xn)

    def mixer_fold():
        arrived(mrc, m_r.at[0])
        mine = (1 - x) * 2 + c
        mp[mine] = (mp[mine].astype(F32) + mrc[1 - x].astype(F32)).astype(BF)

    def mixer_send(h):
        m_x(h).start()

    z_step(1)
    own_x()
    compacts(1)
    z_step(2)
    compacts(2)
    mixer()
    for name in ("eg", "eu", "ed"):
        loads[name].wait()
    compute(order[1])
    few_send(order[1])
    z_step(3)
    compacts(3)
    compute(order[2])
    core_step(z, 2)
    shared()
    experts(z, 2)
    for side in range(2):
        d_core(z, side).start()
    few_send(order[2])
    compute(order[3])
    few_send(order[3])
    mixer_fold()
    mixer_send(0)
    mixer_send(1)
    fold_core()
    fold_z(target(1))
    fold_z(target(2))
    fold_z(target(3))
    for h in range(HALVES):
        m_x(h).wait_recv()
    loads["mgain"].wait()
    mixed = mp[t].astype(F32) + mrc[x].astype(F32) + mrx[...].astype(F32)
    scale = lax.rsqrt(jnp.mean(mixed * mixed, axis=-1, keepdims=True) + EPSILON)
    mixed_ref[...] = (mixed * scale * mgain[...]).astype(BF)

    here = lines(z, 0, c)
    d_core(z, 0).wait_recv()
    for p in range(PARTS):
        band = cols(p)
        d_x(p).wait_recv()
        total = dd[here, band].astype(F32) + rc[z, :, band].astype(F32) + rx[:, band].astype(F32)

        last_arrival(1, p).wait_recv()
        total = total + last_in[1, :, band].astype(F32)

        @pl.when(is_edge)
        def _():
            last_arrival(0, p).wait_recv()
            rows_ref[:, band] = (total + last_in[0, :, band].astype(F32)).astype(BF)

        @pl.when(jnp.logical_not(is_edge))
        def _():
            to_inner(z, p).wait_recv()
            rows_ref[:, band] = (total + edge_in[z, :, band].astype(F32)).astype(BF)

    def left(ref, sem):
        rcopy(ref, ref, sem, m_r.at[0], xn).wait_send()

    def drain():
        @pl.when(has_up)
        def _():
            left(halo, sent.at[3])

        for edge_chip, moved in ((True, 1), (False, 2 * ep - 3)):
            total_blocks = moved + ep + 2

            @pl.when(is_edge == edge_chip)
            def _():
                left(gat.at[pl.ds(0, total_blocks * rows), :], sent.at[0])
                left(tab.at[pl.ds(0, total_blocks)], sent.at[0])

        slots = 2 * (ep - 1) * 2 * cap
        left(gat.at[pl.ds(0, slots + (ep + 1) * rows), :], sent.at[1])
        left(gat.at[pl.ds(0, (1 + ep - 1 + 3) * rows), :], sent.at[2])

    drain()


def store_rows(mixed_ref, rows_ref, mixed_out, rows_out, sem):
    copies = [
        pltpu.make_async_copy(mixed_ref, mixed_out, sem.at[0]),
        pltpu.make_async_copy(rows_ref, rows_out, sem.at[1]),
    ]
    for copy in copies:
        copy.start()
    for copy in copies:
        copy.wait()


def fused_on_device(ep, tp, *args):
    (og, ig, iv, taps, mo, mgain, tok, egain, ids, wts, eg, eu, ed, sg, su, sd) = args
    rows, width = tok.shape
    count, columns = ig.shape
    experts = ep * tp
    cap = (3 * rows * ids.shape[1] + 2 * experts - 1) // (2 * experts)
    cap = -(-cap // 8) * 8
    slot = -(-cap // 32) * 32
    names = -(-experts // 16) * 16
    hid = eg.shape[2]
    half = sd.shape[0]
    any_spec = pl.BlockSpec(memory_space=pltpu.HBM)
    vmem = pl.BlockSpec(memory_space=pltpu.VMEM)
    dma = pltpu.SemaphoreType.DMA
    V = pltpu.VMEM
    mixed, summed = pl.pallas_call(
        functools.partial(fused_kernel, ep, tp, cap, slot),
        out_shape=(V((rows, width), BF), V((rows, width), BF)),
        in_specs=[any_spec] * 16,
        out_specs=(vmem, vmem),
        scratch_shapes=[
            V((count, columns), BF), V((count, columns), BF), V((count, columns), BF),
            V((columns, width), BF), V((rows, width), BF),
            V(taps.shape, BF), V((1, width), F32), V((1, width), F32),
            V(ids.shape[::-1], jnp.int32), V(wts.shape[::-1], F32),
            V((width, hid), BF), V((width, hid), BF), V((hid + half, width), BF),
            V((width, 2 * half), BF),
            V((2, 16, columns), BF), V((count + 8, columns), F32), V((count, columns), BF),
            V((experts * rows, width), BF), V((experts, names, 128), BF),
            V((tp * rows, hid + half), BF), V((experts * rows, width), BF),
            V((ep, 2 * slot, width), BF), V((ep, 2 * slot, 128), BF),
            V((ep + 1, rows, width), BF), V((ep, 2 * slot, width), BF), V((rows, width), BF),
            V((ep, rows, width), BF), V((2, rows, width), BF),
            V((tp, rows, width), BF), V((2, rows, width), BF), V((rows, width), BF),
            dma((16,)), dma((2,)), dma((ep, CHUNKS + 1)), dma((CHUNKS + 1,)), dma((ep + 1, 2)), dma((ep,)),
            dma((ep + 1,)), dma((ep, HALVES)), dma((PARTS,)), dma((ep, PARTS)), dma((2, PARTS)),
            dma((1 + HALVES,)), dma((4,)),
        ],
        compiler_params=pltpu.CompilerParams(
            collective_id=0, has_side_effects=True, vmem_limit_bytes=60 * 1024 * 1024
        ),
    )(
        og, ig, iv, taps, mo, mgain.reshape(1, -1), tok, egain.reshape(1, -1), ids.T, wts.T, eg, eu, ed, sg, su, sd
    )
    out = jax.ShapeDtypeStruct((rows, width), BF)
    return pl.pallas_call(
        store_rows,
        out_shape=(out, out),
        in_specs=[vmem, vmem],
        out_specs=(any_spec, any_spec),
        scratch_shapes=[dma((2,))],
    )(
        pltpu.with_memory_space_constraint(mixed, pltpu.VMEM),
        pltpu.with_memory_space_constraint(summed, pltpu.VMEM),
    )


def plan(mesh):
    ep, tp = mesh.shape["ep"], mesh.shape["tp"]
    if tp == 4 and ep == 4:
        return functools.partial(fused_on_device, ep, tp)
    return on_device


def solution(mesh):
    return jax.shard_map(
        plan(mesh),
        mesh=mesh,
        in_specs=(
            P(("grp", "ep"), "tp"),
            P(("grp", "ep"), "tp"),
            P(("grp", "ep"), "tp"),
            P(),
            P("tp", None),
            P(),
            P(("grp", "ep", "tp"), None),
            P(),
            P(("grp", "ep", "tp"), None),
            P(("grp", "ep", "tp"), None),
            P(("ep", "tp"), None, None),
            P(("ep", "tp"), None, None),
            P(("ep", "tp"), None, None),
            P(None, "tp"),
            P(None, "tp"),
            P("tp", None),
        ),
        out_specs=(P(("grp", "ep", "tp"), None), P(("grp", "ep", "tp"), None)),
        check_vma=False,
    )
```

```python
import functools
import jax
import jax.numpy as jnp
from jax import lax
from jax.experimental import pallas as pl
from jax.experimental.pallas import tpu as pltpu
from jax.sharding import PartitionSpec as P

EPSILON = 1e-06


def passed_along(array, axis, by):
    size = lax.axis_size(axis)
    pairs = [(i, i + by) for i in range(size) if 0 <= i + by < size]
    return lax.ppermute(array, axis, pairs)


def rms_scale(values, gains):
    return values * lax.rsqrt(jnp.mean(values * values, axis=-1, keepdims=True) + EPSILON) * gains


def on_device(
    outer_gate,
    inner_gate,
    inner_value,
    conv_taps,
    mixer_out,
    mixer_gain,
    moe_tokens,
    expert_gain,
    route_ids,
    route_weights,
    expert_gate,
    expert_up,
    expert_down,
    shared_gate,
    shared_up,
    shared_down,
):
    columns = inner_gate.shape[1]
    kernel = lax.dynamic_slice_in_dim(conv_taps, lax.axis_index("tp") * columns, columns, 1).astype(
        jnp.float32
    )
    before_gate, before_value = passed_along((inner_gate[-2:], inner_value[-2:]), "ep", 1)
    gate_rows = jnp.concatenate([before_gate, inner_gate], axis=0).astype(jnp.float32)
    value_rows = jnp.concatenate([before_value, inner_value], axis=0).astype(jnp.float32)
    product = gate_rows * value_rows
    filtered = kernel[0] * product[:-2] + kernel[1] * product[1:-1] + kernel[2] * product[2:]
    scaled = (outer_gate.astype(jnp.float32) * filtered).astype(jnp.bfloat16)
    normed = rms_scale(moe_tokens.astype(jnp.float32), expert_gain).astype(jnp.bfloat16)
    feature_width = normed.shape[1]
    piece = lax.all_gather(normed, "tp", axis=0, tiled=True)
    gate_value = jnp.dot(piece, shared_gate, preferred_element_type=jnp.float32)
    up_value = jnp.dot(piece, shared_up, preferred_element_type=jnp.float32)
    shared_act = (jax.nn.silu(gate_value) * up_value).astype(jnp.bfloat16)
    mixer_part = jnp.dot(scaled, mixer_out, preferred_element_type=jnp.float32)
    shared_part = jnp.dot(shared_act, shared_down, preferred_element_type=jnp.float32)
    both_sums = lax.psum_scatter(
        jnp.concatenate([mixer_part, shared_part], axis=1).astype(jnp.bfloat16),
        "tp",
        scatter_dimension=0,
        tiled=True,
    ).astype(jnp.float32)
    mixed_rows = rms_scale(both_sums[:, :feature_width], mixer_gain).astype(jnp.bfloat16)
    shared_out = both_sums[:, feature_width:]
    row_count, top_count = route_ids.shape
    ep_count = lax.axis_size("ep")
    tp_count = lax.axis_size("tp")
    expert_count = ep_count * tp_count
    capacity = (3 * row_count * top_count + 2 * expert_count - 1) // (2 * expert_count)
    flat_ids = route_ids.reshape(-1)
    onehot = (flat_ids[:, None] == jnp.arange(expert_count, dtype=jnp.int32)[None, :]).astype(
        jnp.int32
    )
    slot_rank = jnp.sum(
        (jnp.cumsum(onehot, axis=0, dtype=jnp.int32) - onehot) * onehot, axis=1, dtype=jnp.int32
    )
    target = flat_ids * capacity + slot_rank
    token_of = jnp.arange(flat_ids.shape[0], dtype=jnp.int32) // top_count
    slot_token = jnp.zeros((expert_count * capacity,), jnp.int32).at[target].set(token_of)
    outgoing = normed[slot_token].reshape(expert_count, capacity, feature_width)
    arrived = lax.all_to_all(outgoing, ("ep", "tp"), split_axis=0, concat_axis=0, tiled=True)
    flat_in = arrived.reshape(expert_count * capacity, feature_width)
    gate_value = jnp.dot(flat_in, expert_gate[0], preferred_element_type=jnp.float32)
    up_value = jnp.dot(flat_in, expert_up[0], preferred_element_type=jnp.float32)
    active = (jax.nn.silu(gate_value) * up_value).astype(jnp.bfloat16)
    result = jnp.dot(active, expert_down[0], preferred_element_type=jnp.float32).astype(
        jnp.bfloat16
    )
    returned = lax.all_to_all(
        result.reshape(expert_count, capacity, feature_width),
        ("ep", "tp"),
        split_axis=0,
        concat_axis=0,
        tiled=True,
    )
    picked = returned.reshape(expert_count * capacity, feature_width)[target].astype(jnp.float32)
    weights = route_weights.reshape(-1)
    routed = jnp.sum(
        (weights[:, None] * picked).reshape(row_count, top_count, feature_width), axis=1
    )
    expert_rows = (shared_out + routed).astype(jnp.bfloat16)
    return (mixed_rows, expert_rows)


MESH = pl.DeviceIdType.MESH
BF = jnp.bfloat16
F32 = jnp.float32
CHUNKS = 2
PARTS = 4
HALVES = 2
PIECES = (CHUNKS,) + tuple(range(CHUNKS))


def dot(a, b):
    return jnp.dot(a, b, preferred_element_type=F32)


def dot_rows(a, b):
    return lax.dot_general(a, b, (((0,), (0,)), ((), ())), preferred_element_type=F32)


def fused_kernel(
    ep, tp, cap, slot,
    og_h, ig_h, iv_h, taps_h, mo_h, mgain_h, tok_h, egain_h, ids_h, wts_h, eg_h, eu_h, ed_h, sg_h, su_h, sd_h,
    mixed_ref, rows_ref,
    og, ig, iv, mo, tok, taps, mgain, egain, ids, wts, eg, eu, ed, sgu, halo, pbuf, scaled,
    gat, tab, act, dd, packed, spread, rc, back, rx, edge_in, last_in, mp, mrc, mrx,
    load_sem, halo_sem, gz_r, gx_r, gc_r, px_r, rc_r, q_r, rx_r, e_r, f_r, m_r, sent,
):
    z = lax.axis_index("ep")
    t = lax.axis_index("tp")
    g = lax.axis_index("grp")
    x = t // 2
    c = t % 2
    rows = tok.shape[0]
    width = tok.shape[1]
    columns = ig.shape[1]
    sub = rows // CHUNKS
    up = (g, z + 1, t)
    down = (g, z - 1, t)
    xn = (g, z, (1 - x) * 2 + c)
    pc = (g, z, x * 2 + 1 - c)
    xd = (g, z, (1 - x) * 2 + 1 - c)
    z2 = (g, (z + 2) % ep, t)
    is_edge = jnp.logical_or(z == 0, z == ep - 1)
    inner = jnp.where(2 * z < ep, z + 1, z - 1)
    outer = jnp.where(2 * z < ep, z - 1, z + 1)
    has_up = z < ep - 1
    has_down = z > 0

    barrier = pltpu.get_barrier_semaphore()
    for peer in (xn, pc, xd, z2):
        pl.semaphore_signal(barrier, inc=1, device_id=peer, device_id_type=MESH)

    @pl.when(has_up)
    def _():
        pl.semaphore_signal(barrier, inc=1, device_id=up, device_id_type=MESH)

    @pl.when(has_down)
    def _():
        pl.semaphore_signal(barrier, inc=1, device_id=down, device_id_type=MESH)

    loads = {}

    def load(name, src, dst):
        copy = pltpu.make_async_copy(src, dst, load_sem.at[len(loads)])
        copy.start()
        loads[name] = copy

    half = sd_h.shape[0]
    hid = eg.shape[1]
    load("tok", tok_h, tok)
    load("egain", egain_h, egain)
    load("ids", ids_h, ids)
    load("wts", wts_h, wts)
    load("ig", ig_h, ig)
    load("iv", iv_h, iv)
    load("taps", taps_h, taps)
    load("og", og_h, og)
    load("mo", mo_h, mo)
    load("sg", sg_h, sgu.at[:, pl.ds(0, half)])
    load("su", su_h, sgu.at[:, pl.ds(half, half)])
    load("sd", sd_h, ed.at[pl.ds(hid, half), :])
    load("eg", eg_h.at[0], eg)
    load("eu", eu_h.at[0], eu)
    load("ed", ed_h.at[0], ed.at[pl.ds(0, hid), :])
    load("mgain", mgain_h, mgain)

    def rcopy(src, dst, ssem, rsem, peer):
        return pltpu.make_async_remote_copy(
            src_ref=src, dst_ref=dst, send_sem=ssem, recv_sem=rsem, device_id=peer, device_id_type=MESH
        )

    def arrived(ref, sem):
        rcopy(ref, ref, sent.at[0], sem, xn).wait_recv()

    def block(zz, side, cc):
        return (zz * 2 + side) * 2 + cc

    def lines(zz, side, cc):
        return pl.ds(pl.multiple_of(block(zz, side, cc) * rows, rows), rows)

    def few(zz, cc):
        return pl.ds(pl.multiple_of(block(zz, 1, 0) * rows + cc * slot, slot), cap)

    def slots_of(cc):
        return pl.ds(pl.multiple_of(cc * slot, slot), cap)

    def piece(zz, side, cc, k):
        if k == CHUNKS:
            return tab.at[block(zz, side, cc)]
        return gat.at[pl.ds(pl.multiple_of(block(zz, side, cc) * rows + k * sub, sub), sub), :]

    def c_up(zz, k):
        return rcopy(piece(zz, 0, c, k), piece(zz, 0, c, k), sent.at[0], gz_r.at[zz, k], up)

    def c_down(zz, k):
        return rcopy(piece(zz, 0, c, k), piece(zz, 0, c, k), sent.at[0], gz_r.at[zz, k], down)

    def c_x(k):
        return rcopy(piece(z, 0, c, k), piece(z, 1, c, k), sent.at[0], gx_r.at[k], xn)

    def core_pair(zz, side, cc):
        names = tab.at[block(zz, side, cc)]
        body = gat.at[lines(zz, side, cc), :]
        at = zz if side == 0 else ep
        return (
            rcopy(body, body, sent.at[0], gc_r.at[at, 0], pc),
            rcopy(names, names, sent.at[0], gc_r.at[at, 1], pc),
        )

    def core_start(zz, side):
        for copy in core_pair(zz, side, c):
            copy.start()

    def few_pair(zz):
        return (
            rcopy(packed.at[zz, slots_of(c), :], gat.at[few(zz, c), :], sent.at[1], px_r.at[zz], xn),
            rcopy(packed.at[zz, slots_of(1 - c), :], gat.at[few(zz, c), :], sent.at[1], px_r.at[zz], xd),
        )

    for name in ("tok", "egain", "ids", "wts"):
        loads[name].wait()
    name_i = lax.broadcasted_iota(jnp.int32, (tab.shape[1], rows), 0)
    table = jnp.zeros((tab.shape[1], rows), F32)
    for k in range(ids.shape[0]):
        table = table + jnp.where(ids[k : k + 1, :] == name_i, wts[k : k + 1, :], 0.0)
    tab[block(z, 0, c)] = jnp.zeros(tab.shape[1:], BF)
    tab[block(z, 0, c), :, :rows] = table.astype(BF)
    v = tok[...].astype(F32)
    v = v * lax.rsqrt(jnp.mean(v * v, axis=-1, keepdims=True) + EPSILON) * egain[...]
    gat[lines(z, 0, c), :] = v.astype(BF)

    pl.semaphore_wait(barrier, 4 + jnp.minimum(z, 1) + jnp.minimum(ep - 1 - z, 1))

    loads["ig"].wait()
    loads["iv"].wait()
    tail = ig.shape[0] - halo.shape[1]
    edge = halo.shape[1]
    h_gate = rcopy(ig.at[pl.ds(tail, edge)], halo.at[0], sent.at[3], halo_sem.at[0], up)
    h_value = rcopy(iv.at[pl.ds(tail, edge)], halo.at[1], sent.at[3], halo_sem.at[1], up)

    @pl.when(has_up)
    def _():
        h_gate.start()
        h_value.start()

    for k in PIECES:
        @pl.when(has_up)
        def _():
            c_up(z, k).start()

        @pl.when(has_down)
        def _():
            c_down(z, k).start()

        c_x(k).start()
    core_start(z, 0)

    for zz in range(ep):
        for e in range(2):
            back[zz, pl.ds(e * slot + cap, slot - cap), :] = jnp.zeros((slot - cap, width), BF)

    count = ig.shape[0]
    tile = width // PARTS

    def cols(n):
        return pl.ds(pl.multiple_of(n * tile, tile), tile)

    def m_core(xx):
        return rcopy(mp.at[xx * 2 + 1 - c], mrc.at[xx], sent.at[2], m_r.at[0], pc)

    def mixer():
        pbuf[8:, :] = ig[...].astype(F32) * iv[...].astype(F32)

        @pl.when(jnp.logical_not(has_down))
        def _():
            pbuf[:8, :] = jnp.zeros((8, columns), F32)

        @pl.when(has_down)
        def _():
            h_gate.wait_recv()
            h_value.wait_recv()
            pbuf[:8, :] = halo[0, edge - 8 :, :].astype(F32) * halo[1, edge - 8 :, :].astype(F32)

        loads["og"].wait()
        loads["taps"].wait()
        tap = taps[:, pl.ds(pl.multiple_of(t * columns, columns), columns)].astype(F32)
        filtered = (
            tap[0:1] * pbuf[6 : 6 + count, :] + tap[1:2] * pbuf[7 : 7 + count, :] + tap[2:3] * pbuf[8 : 8 + count, :]
        )
        scaled[...] = (og[...].astype(F32) * filtered).astype(BF)
        loads["mo"].wait()
        @pl.loop(0, PARTS, unroll=True)
        def _(n):
            part = dot(scaled[...], mo[:, cols(n)]).astype(BF)
            mp[:, :, cols(n)] = part.reshape(tp, rows, tile)

        for xx in range(2):
            m_core(xx).start()

    lanes = tab.shape[2]
    name_of = lax.broadcasted_iota(jnp.int32, (tab.shape[1], lanes), 0)
    before = (
        lax.broadcasted_iota(jnp.int32, (lanes, lanes), 0) < lax.broadcasted_iota(jnp.int32, (lanes, lanes), 1)
    ).astype(BF)
    slot_i = lax.broadcasted_iota(jnp.int32, (slot, lanes), 0)
    diagonal = lax.broadcasted_iota(jnp.int32, (rows, lanes), 0) == lax.broadcasted_iota(
        jnp.int32, (rows, lanes), 1
    )
    expert = z * tp + t

    def line_of(name, block_id):
        return jnp.sum(jnp.where(name_of == name, tab[block_id].astype(F32), 0.0), axis=0, keepdims=True)

    def weight_column(block_id):
        return jnp.sum(jnp.where(diagonal, line_of(expert, block_id), 0.0), axis=1, keepdims=True)

    def compact(zz):
        marks = []
        for e in range(2):
            weight = line_of(z * tp + (1 - x) * 2 + e, block(zz, 0, c))
            named = weight > 0
            ahead = dot(jnp.broadcast_to(named, (8, lanes)).astype(F32).astype(BF), before)[0:1]
            hit = jnp.logical_and(slot_i == ahead.astype(jnp.int32), named)
            marks.append(hit.astype(F32))
            spread[zz, pl.ds(e * slot, slot), :] = jnp.where(hit, weight, 0.0).astype(BF)
        mark = jnp.concatenate(marks, axis=0).astype(BF)[:, :rows]

        @pl.loop(0, PARTS, unroll=True)
        def _(n):
            packed[zz, :, cols(n)] = dot(mark, gat[lines(zz, 0, c), cols(n)]).astype(BF)

        for copy in few_pair(zz):
            copy.start()

    def z_step(s):
        for k in PIECES:
            @pl.when(z >= s)
            def _():
                c_up(z - s, k).wait_recv()

                @pl.when(has_up)
                def _():
                    c_up(z - s, k).start()

            @pl.when(z + s < ep)
            def _():
                c_down(z + s, k).wait_recv()

                @pl.when(has_down)
                def _():
                    c_down(z + s, k).start()

        @pl.when(z >= s)
        def _():
            core_start(z - s, 0)

        @pl.when(z + s < ep)
        def _():
            core_start(z + s, 0)

    def compacts(s):
        @pl.when(z >= s)
        def _():
            compact(z - s)

        @pl.when(z + s < ep)
        def _():
            compact(z + s)

    def own_x():
        for k in PIECES:
            c_x(k).wait_recv()
        core_start(z, 1)

    def core_step(zz, sides):
        for side in range(sides):
            for copy in core_pair(zz, side, 1 - c):
                copy.wait_recv()
        if sides == 1:
            arrived(gat.at[pl.ds(pl.multiple_of(block(zz, 1, 0) * rows, rows), 2 * cap), :], px_r.at[zz])

    def nth(n):
        near = jnp.minimum(z, ep - 1 - z)
        d = (n + 1) // 2
        side = z - d if n % 2 else z + d
        far = jnp.where(z < ep - 1 - z, n, ep - 1 - n)
        return jnp.where(n <= 2 * near, side, far)

    order = [nth(n) for n in range(ep)]

    def shared():
        for name in ("sg", "su", "sd"):
            loads[name].wait()
        own = pl.ds(pl.multiple_of(block(z, 0, 0) * rows, tp * rows), tp * rows)
        hidden = dot(gat[own, :], sgu[...])
        gate, value = hidden[:, :half], hidden[:, half:]
        act[:, hid:] = (gate / (1.0 + jnp.exp(-gate)) * value).astype(BF)

    def experts(zz, sides):
        depth = hid + half if sides == 2 else hid
        weights = [weight_column(block(zz, side, cc)) for side in range(sides) for cc in range(2)]
        if sides == 1:
            weights.append(jnp.ones((2 * slot, 1), F32))
        weight = jnp.concatenate(weights, axis=0)
        amount = weight.shape[0]
        span = pl.ds(pl.multiple_of(block(zz, 0, 0) * rows, tp * rows), amount)
        step = 256 if hid % 256 == 0 else hid

        @pl.loop(0, hid // step, unroll=True)
        def _(n):
            col = pl.ds(pl.multiple_of(n * step, step), step)
            gate = dot(gat[span, :], eg[:, col])
            value = dot(gat[span, :], eu[:, col])
            act[:amount, col] = (gate / (1.0 + jnp.exp(-gate)) * value * weight).astype(BF)

        @pl.loop(0, PARTS, unroll=True)
        def _(n):
            dd[span, cols(n)] = dot(act[:amount, :depth], ed[:depth, cols(n)]).astype(BF)

    def d_core(zz, side):
        at = zz if side == 0 else ep
        return rcopy(dd.at[lines(zz, side, 1 - c), :], rc.at[at], sent.at[1], rc_r.at[at], pc)

    wide = width // HALVES

    def d_few(zz, h):
        part = pl.ds(h * wide, wide)
        return (
            rcopy(
                dd.at[few(zz, c), part], back.at[zz, slots_of(c), part],
                sent.at[1], q_r.at[zz, h], xn,
            ),
            rcopy(
                dd.at[few(zz, 1 - c), part], back.at[zz, slots_of(c), part],
                sent.at[1], q_r.at[zz, h], xd,
            ),
        )

    def d_x(p):
        return rcopy(dd.at[lines(z, 1, c), cols(p)], rx.at[:, cols(p)], sent.at[2], rx_r.at[p], xn)

    def to_inner(zz, p):
        src = dd.at[lines(zz, 0, c), cols(p)]
        return rcopy(src, edge_in.at[zz, :, cols(p)], sent.at[2], e_r.at[zz, p], (g, inner, t))

    def to_owner(zz, p):
        owner_is_edge = jnp.logical_or(zz == 0, zz == ep - 1)
        place = jnp.where(jnp.logical_and(owner_is_edge, zz == outer), 0, 1)
        src = dd.at[lines(zz, 0, c), cols(p)]
        return rcopy(src, last_in.at[place, :, cols(p)], sent.at[2], f_r.at[place, p], (g, zz, t))

    def last_arrival(place, p):
        here = last_in.at[place, :, cols(p)]
        return rcopy(here, here, sent.at[2], f_r.at[place, p], xn)

    def compute(zz):
        core_step(zz, 1)
        experts(zz, 1)
        d_core(zz, 0).start()

    def few_send(zz):
        for h in range(HALVES):
            for copy in d_few(zz, h):
                copy.start()

    def fold_core():
        d_core(z, 1).wait_recv()
        there = lines(z, 1, c)
        dd[there, :] = (dd[there, :].astype(F32) + rc[ep].astype(F32)).astype(BF)
        for p in range(PARTS):
            d_x(p).start()

    def fold_z(zz):
        here = lines(zz, 0, c)
        d_core(zz, 0).wait_recv()
        for p in range(PARTS):
            band = cols(p)
            if p % (PARTS // HALVES) == 0:
                h = p // (PARTS // HALVES)
                arrived(back.at[zz, pl.ds(0, 2 * cap), pl.ds(h * wide, wide)], q_r.at[zz, h])
            so_far = (
                dd[here, band].astype(F32)
                + rc[zz, :, band].astype(F32)
                + dot_rows(spread[zz], back[zz, :, band])[:rows]
            )

            @pl.when(jnp.logical_or(is_edge, zz == outer))
            def _():
                dd[here, band] = so_far.astype(BF)

            @pl.when(jnp.logical_not(jnp.logical_or(is_edge, zz == outer)))
            def _():
                to_inner(zz, p).wait_recv()
                dd[here, band] = (so_far + edge_in[zz, :, band].astype(F32)).astype(BF)

            @pl.when(is_edge)
            def _():
                to_inner(zz, p).start()

            @pl.when(jnp.logical_not(is_edge))
            def _():
                to_owner(zz, p).start()

    def target(n):
        edge_first, inner_first = ((2, 3, 1), (0, 2, 3))
        found = jnp.where(is_edge, edge_first[n - 1], inner_first[n - 1])
        return jnp.where(2 * z < ep, found, ep - 1 - found)

    def m_x(h):
        part = pl.ds(h * wide, wide)
        return rcopy(mp.at[(1 - x) * 2 + c, :, part], mrx.at[:, part], sent.at[2], m_r.at[1 + h], xn)

    def mixer_fold():
        arrived(mrc, m_r.at[0])
        mine = (1 - x) * 2 + c
        mp[mine] = (mp[mine].astype(F32) + mrc[1 - x].astype(F32)).astype(BF)

    def mixer_send(h):
        m_x(h).start()

    z_step(1)
    own_x()
    compacts(1)
    z_step(2)
    compacts(2)
    mixer()
    for name in ("eg", "eu", "ed"):
        loads[name].wait()
    compute(order[1])
    few_send(order[1])
    z_step(3)
    compacts(3)
    compute(order[2])
    core_step(z, 2)
    shared()
    experts(z, 2)
    for side in range(2):
        d_core(z, side).start()
    few_send(order[2])
    compute(order[3])
    few_send(order[3])
    mixer_fold()
    mixer_send(0)
    mixer_send(1)
    fold_core()
    fold_z(target(1))
    fold_z(target(2))
    fold_z(target(3))
    for h in range(HALVES):
        m_x(h).wait_recv()
    loads["mgain"].wait()
    mixed = mp[t].astype(F32) + mrc[x].astype(F32) + mrx[...].astype(F32)
    scale = lax.rsqrt(jnp.mean(mixed * mixed, axis=-1, keepdims=True) + EPSILON)
    mixed_ref[...] = (mixed * scale * mgain[...]).astype(BF)

    here = lines(z, 0, c)
    d_core(z, 0).wait_recv()
    for p in range(PARTS):
        band = cols(p)
        d_x(p).wait_recv()
        total = dd[here, band].astype(F32) + rc[z, :, band].astype(F32) + rx[:, band].astype(F32)

        last_arrival(1, p).wait_recv()
        total = total + last_in[1, :, band].astype(F32)

        @pl.when(is_edge)
        def _():
            last_arrival(0, p).wait_recv()
            rows_ref[:, band] = (total + last_in[0, :, band].astype(F32)).astype(BF)

        @pl.when(jnp.logical_not(is_edge))
        def _():
            to_inner(z, p).wait_recv()
            rows_ref[:, band] = (total + edge_in[z, :, band].astype(F32)).astype(BF)

    def left(ref, sem):
        rcopy(ref, ref, sem, m_r.at[0], xn).wait_send()

    def drain():
        @pl.when(has_up)
        def _():
            left(halo, sent.at[3])

        for edge_chip, moved in ((True, 1), (False, 2 * ep - 3)):
            total_blocks = moved + ep + 2

            @pl.when(is_edge == edge_chip)
            def _():
                left(gat.at[pl.ds(0, total_blocks * rows), :], sent.at[0])
                left(tab.at[pl.ds(0, total_blocks)], sent.at[0])

        slots = 2 * (ep - 1) * 2 * cap
        left(gat.at[pl.ds(0, slots + (ep + 1) * rows), :], sent.at[1])
        left(gat.at[pl.ds(0, (1 + ep - 1 + 3) * rows), :], sent.at[2])

    drain()


def store_rows(mixed_ref, rows_ref, mixed_out, rows_out, sem):
    copies = [
        pltpu.make_async_copy(mixed_ref, mixed_out, sem.at[0]),
        pltpu.make_async_copy(rows_ref, rows_out, sem.at[1]),
    ]
    for copy in copies:
        copy.start()
    for copy in copies:
        copy.wait()


def fused_on_device(ep, tp, *args):
    (og, ig, iv, taps, mo, mgain, tok, egain, ids, wts, eg, eu, ed, sg, su, sd) = args
    rows, width = tok.shape
    count, columns = ig.shape
    experts = ep * tp
    cap = (3 * rows * ids.shape[1] + 2 * experts - 1) // (2 * experts)
    cap = -(-cap // 8) * 8
    slot = -(-cap // 32) * 32
    names = -(-experts // 16) * 16
    hid = eg.shape[2]
    half = sd.shape[0]
    any_spec = pl.BlockSpec(memory_space=pltpu.HBM)
    vmem = pl.BlockSpec(memory_space=pltpu.VMEM)
    dma = pltpu.SemaphoreType.DMA
    V = pltpu.VMEM
    mixed, summed = pl.pallas_call(
        functools.partial(fused_kernel, ep, tp, cap, slot),
        out_shape=(V((rows, width), BF), V((rows, width), BF)),
        in_specs=[any_spec] * 16,
        out_specs=(vmem, vmem),
        scratch_shapes=[
            V((count, columns), BF), V((count, columns), BF), V((count, columns), BF),
            V((columns, width), BF), V((rows, width), BF),
            V(taps.shape, BF), V((1, width), F32), V((1, width), F32),
            V(ids.shape[::-1], jnp.int32), V(wts.shape[::-1], F32),
            V((width, hid), BF), V((width, hid), BF), V((hid + half, width), BF),
            V((width, 2 * half), BF),
            V((2, 16, columns), BF), V((count + 8, columns), F32), V((count, columns), BF),
            V((experts * rows, width), BF), V((experts, names, 128), BF),
            V((tp * rows, hid + half), BF), V((experts * rows, width), BF),
            V((ep, 2 * slot, width), BF), V((ep, 2 * slot, 128), BF),
            V((ep + 1, rows, width), BF), V((ep, 2 * slot, width), BF), V((rows, width), BF),
            V((ep, rows, width), BF), V((2, rows, width), BF),
            V((tp, rows, width), BF), V((2, rows, width), BF), V((rows, width), BF),
            dma((16,)), dma((2,)), dma((ep, CHUNKS + 1)), dma((CHUNKS + 1,)), dma((ep + 1, 2)), dma((ep,)),
            dma((ep + 1,)), dma((ep, HALVES)), dma((PARTS,)), dma((ep, PARTS)), dma((2, PARTS)),
            dma((1 + HALVES,)), dma((4,)),
        ],
        compiler_params=pltpu.CompilerParams(
            collective_id=0, has_side_effects=True, vmem_limit_bytes=60 * 1024 * 1024
        ),
    )(
        og, ig, iv, taps, mo, mgain.reshape(1, -1), tok, egain.reshape(1, -1), ids.T, wts.T, eg, eu, ed, sg, su, sd
    )
    out = jax.ShapeDtypeStruct((rows, width), BF)
    return pl.pallas_call(
        store_rows,
        out_shape=(out, out),
        in_specs=[vmem, vmem],
        out_specs=(any_spec, any_spec),
        scratch_shapes=[dma((2,))],
    )(
        pltpu.with_memory_space_constraint(mixed, pltpu.VMEM),
        pltpu.with_memory_space_constraint(summed, pltpu.VMEM),
    )


def plan(mesh):
    ep, tp = mesh.shape["ep"], mesh.shape["tp"]
    if tp == 4 and ep == 4:
        return functools.partial(fused_on_device, ep, tp)
    return on_device


def solution(mesh):
    return jax.shard_map(
        plan(mesh),
        mesh=mesh,
        in_specs=(
            P(("grp", "ep"), "tp"),
            P(("grp", "ep"), "tp"),
            P(("grp", "ep"), "tp"),
            P(),
            P("tp", None),
            P(),
            P(("grp", "ep", "tp"), None),
            P(),
            P(("grp", "ep", "tp"), None),
            P(("grp", "ep", "tp"), None),
            P(("ep", "tp"), None, None),
            P(("ep", "tp"), None, None),
            P(("ep", "tp"), None, None),
            P(None, "tp"),
            P(None, "tp"),
            P("tp", None),
        ),
        out_specs=(P(("grp", "ep", "tp"), None), P(("grp", "ep", "tp"), None)),
        check_vma=False,
    )
```
